512 devices in a mesh: grp: 2 (over y), fs: 32 (over z), tp: 8 (over x, core).
Axes of the slice: x: 4, y: 2, z: 32, core: 2. Of those that a mesh axis runs over, the one named last changes fastest.
The devices are a block of a 4x8x32 slice.
Arguments:
- tokens: bfloat16 [16384, 2048], P(('grp', 'fs'), 'tp'), parts along dimension 0, may hold values from -6 to 6
- recurrent_norm_gain: float32 [2048], replicated, may hold values from 0.1 to 1.9
- feedforward_norm_gain: float32 [2048], replicated, may hold values from 0.1 to 1.9
- gate_projection_weight: bfloat16 [2048, 2048], P('fs', 'tp'), may hold values from -0.125 to 0.125
- recurrent_projection_weight: bfloat16 [2048, 2048], P('fs', 'tp'), may hold values from -0.125 to 0.125
- convolution_kernel: bfloat16 [4, 2048], P(None, 'tp'), may hold values from -3 to 3
- decay_gate_matrix: bfloat16 [16, 128, 128], P('tp'), may hold values from -0.5 to 0.5
- input_gate_matrix: bfloat16 [16, 128, 128], P('tp'), may hold values from -0.5 to 0.5
- base_decay_logit: float32 [2048], P('tp'), may hold values from 3 to 9
- extra_log_decay: float32 [16384], P(('grp', 'fs')), parts along dimension 0, may hold values from -0.7 to 0
- output_projection_weight: bfloat16 [2048, 2048], P('tp', 'fs'), may hold values from -0.125 to 0.125
- up_projection_weight: bfloat16 [2048, 8192], P('fs', 'tp'), may hold values from -0.125 to 0.125
- down_projection_weight: bfloat16 [8192, 2048], P('tp', 'fs'), may hold values from -0.0625 to 0.0625
Outputs:
- layer_out: bfloat16 [16384, 2048], P(('grp', 'fs'), 'tp'), parts along dimension 0
The draws below stay inside these ranges and needn't reach their ends.
There are 2 independent parts, one for each index of `grp`. The reference program is written for one: setup_inputs(seed, part) draws one part's arguments, and reference() takes and returns one part's arrays. A program takes and returns all parts, laid end to end along the dimension named above; an argument that names none is the same for every part. Nothing has to cross between parts.
All inputs are finite; a program needn't handle non-finite values.
Results may differ from the reference program's by a relative error of at most 0.018.
Values may be sent and summed in bfloat16 or wider, within the bound.
No kernel may reach another device: no remote copies, remote signals or barrier semaphores. Data moves between devices by JAX's collectives and lax.ppermute only.
A program may use at most 64 MiB of HBM per device.

```python
import math
import jax
import jax.numpy as jnp
from jax import lax

D = 2048
FF = 8192
BLOCKS = 16
BLOCK_DIM = 128
CONV = 4
SEQUENCE_TOKENS = 256
WIDTH = 2048
TOKENS = 8192
N_TP = 8


def draw_base_decay_logit(key, part):
    key_pick, key_slow, key_fast = jax.random.split(key, 3)
    share = 0.5
    chosen = jax.random.uniform(key_pick, (WIDTH,), jnp.float32) < share
    slow_rate = jnp.exp(jax.random.uniform(key_slow, (WIDTH,), jnp.float32, math.log(0.3), math.log(1.5))) / (4.0 * SEQUENCE_TOKENS)
    fast_rate = 0.25 / jnp.exp(jax.random.uniform(key_fast, (WIDTH,), jnp.float32, math.log(8.0), math.log(25.0)))
    decay_rate = jnp.where(chosen, fast_rate, slow_rate)
    return (-decay_rate - jnp.log(-jnp.expm1(-decay_rate))).astype(jnp.float32)


def draw_extra_log_decay(key, part):
    key_pick, key_depth = jax.random.split(key)
    picked = jax.random.randint(key_pick, (TOKENS,), 0, SEQUENCE_TOKENS) < 3
    depth = jnp.log(jax.random.uniform(key_depth, (TOKENS,), jnp.float32, 0.5, 0.8))
    return jnp.where(picked, depth, 0.0).astype(jnp.float32)


def block_levels(stream_key, shape, cuts, low, largest):
    gain, own = 1.0, jax.random.fold_in(stream_key, 6)
    for axis_at, shards_of in cuts:
        steps = jnp.exp(jax.random.uniform(jax.random.fold_in(own, axis_at), (shards_of,), jnp.float32, low / len(cuts), largest / len(cuts)))
        gain = gain * jnp.repeat(steps, shape[axis_at] // shards_of).reshape([-1 if axis == axis_at else 1 for axis in range(len(shape))])
    return gain


def noise(rng, shape, spread, bound, pieces=(), dtype=jnp.bfloat16):
    drawn = spread * jax.random.normal(rng, shape, jnp.float32)
    if pieces:
        drawn = drawn * block_levels(rng, shape, pieces, -0.22, 0.18)
    return jnp.clip(drawn, -bound, bound).astype(dtype)


def setup_inputs(seed: int = 0, part: int = 0) -> dict:
    key_list = jax.random.split(jax.random.key(seed), 14)
    part_keys = jax.random.split(jax.random.fold_in(key_list[13], part), 14)
    tokens = noise(part_keys[0], (TOKENS, D), 1.0, 6.0, ((0, 32), (1, 8)))
    recurrent_norm_gain = jnp.clip(1.0 + 0.18 * jax.random.normal(key_list[1], (D,), jnp.float32), 0.1, 1.9)
    feedforward_norm_gain = jnp.clip(1.0 + 0.18 * jax.random.normal(key_list[2], (D,), jnp.float32), 0.1, 1.9)
    gate_projection_weight = noise(key_list[3], (D, WIDTH), D ** -0.5, 0.125, ((0, 32), (1, 8)))
    recurrent_projection_weight = noise(key_list[4], (D, WIDTH), D ** -0.5, 0.125, ((0, 32), (1, 8)))
    convolution_kernel = noise(key_list[5], (CONV, WIDTH), 0.5, 3.0, ((1, 8),))
    decay_gate_matrix = noise(key_list[6], (BLOCKS, BLOCK_DIM, BLOCK_DIM), BLOCK_DIM ** -0.5, 0.5, ((0, 8),))
    input_gate_matrix = noise(key_list[7], (BLOCKS, BLOCK_DIM, BLOCK_DIM), BLOCK_DIM ** -0.5, 0.5, ((0, 8),))
    base_decay_logit = draw_base_decay_logit(jax.random.fold_in(key_list[13], 71), part)
    extra_log_decay = draw_extra_log_decay(jax.random.fold_in(jax.random.fold_in(key_list[13], part), 71), part)
    output_projection_weight = noise(key_list[10], (WIDTH, D), WIDTH ** -0.5, 0.125, ((0, 8), (1, 32)))
    up_projection_weight = noise(key_list[11], (D, FF), D ** -0.5, 0.125, ((0, 32), (1, 8)))
    down_projection_weight = noise(key_list[12], (FF, D), FF ** -0.5, 0.0625, ((0, 8), (1, 32)))
    return dict(tokens=tokens, recurrent_norm_gain=recurrent_norm_gain, feedforward_norm_gain=feedforward_norm_gain, gate_projection_weight=gate_projection_weight, recurrent_projection_weight=recurrent_projection_weight, convolution_kernel=convolution_kernel, decay_gate_matrix=decay_gate_matrix, input_gate_matrix=input_gate_matrix, base_decay_logit=base_decay_logit, extra_log_decay=extra_log_decay, output_projection_weight=output_projection_weight, up_projection_weight=up_projection_weight, down_projection_weight=down_projection_weight)


def rms_rows(values_in, norm_gain):
    values = values_in.astype(jnp.float32)
    inverse = lax.rsqrt(lax.optimization_barrier(jnp.mean(values * values, axis=-1, keepdims=True)) + 1e-06)
    return (values * inverse * norm_gain.astype(jnp.float32)).astype(jnp.bfloat16)

def combine(earlier, later):
    return (earlier[0] * later[0], later[0] * earlier[1] + later[1])

def recurrent_state(recurrent_branch_rows, gate_branch_rows, convolution_kernel, decay_gate_matrix, input_gate_matrix, base_decay_logit, extra_log_decay):
    length = recurrent_branch_rows.shape[0]
    taps = convolution_kernel.shape[0]
    padded = jnp.pad(recurrent_branch_rows.astype(jnp.float32), ((taps - 1, 0), (0, 0)))
    conv_sum = jnp.zeros((length, recurrent_branch_rows.shape[1]), jnp.float32)
    for tap_index in range(taps):
        conv_sum = conv_sum + padded[tap_index:tap_index + length] * convolution_kernel[tap_index].astype(jnp.float32)
    conv_rows = conv_sum.astype(jnp.bfloat16)
    blocks = decay_gate_matrix.shape[0]
    blocked = conv_rows.reshape(length, blocks, -1).astype(jnp.float32)
    recurrence_gate = jax.nn.sigmoid(jnp.einsum('tni,nij->tnj', blocked, decay_gate_matrix.astype(jnp.float32)).reshape(length, -1))
    input_rate = jax.nn.sigmoid(jnp.einsum('tni,nij->tnj', blocked, input_gate_matrix.astype(jnp.float32)).reshape(length, -1))
    decay_log_values = -8.0 * jax.nn.softplus(-base_decay_logit) * recurrence_gate + extra_log_decay[:, None]
    decay = jnp.exp(decay_log_values)
    drive = jnp.sqrt(-jnp.expm1(2.0 * decay_log_values)) * input_rate * conv_rows.astype(jnp.float32)
    _, hidden = lax.associative_scan(combine, (decay, drive), axis=0)
    return (hidden * gate_branch_rows.astype(jnp.float32)).astype(jnp.bfloat16)

def split_sum(left_rows, weight):
    block_width = weight.shape[0] // N_TP
    summed = jnp.zeros((left_rows.shape[0], weight.shape[1]), jnp.float32)
    for block_index in range(N_TP):
        lower = block_index * block_width
        partial_value = jnp.dot(left_rows[:, lower:lower + block_width], weight[lower:lower + block_width], preferred_element_type=jnp.float32).astype(jnp.bfloat16)
        summed = summed + lax.optimization_barrier(partial_value).astype(jnp.float32)
    return summed

def reference(tokens, recurrent_norm_gain, feedforward_norm_gain, gate_projection_weight, recurrent_projection_weight, convolution_kernel, decay_gate_matrix, input_gate_matrix, base_decay_logit, extra_log_decay, output_projection_weight, up_projection_weight, down_projection_weight):
    sequence_count = tokens.shape[0]
    sequence_batch = sequence_count // SEQUENCE_TOKENS
    normed = rms_rows(tokens, recurrent_norm_gain)
    gate_branch_rows = jax.nn.gelu(jnp.dot(normed, gate_projection_weight, preferred_element_type=jnp.float32)).astype(jnp.bfloat16)
    recurrent_branch_rows = jnp.dot(normed, recurrent_projection_weight, preferred_element_type=jnp.float32).astype(jnp.bfloat16)
    mixed_output = jax.vmap(recurrent_state, in_axes=(0, 0, None, None, None, None, 0))(recurrent_branch_rows.reshape(sequence_batch, SEQUENCE_TOKENS, -1), gate_branch_rows.reshape(sequence_batch, SEQUENCE_TOKENS, -1), convolution_kernel, decay_gate_matrix, input_gate_matrix, base_decay_logit, extra_log_decay.reshape(sequence_batch, SEQUENCE_TOKENS)).reshape(sequence_count, -1)
    residual = (tokens.astype(jnp.float32) + split_sum(mixed_output, output_projection_weight)).astype(jnp.bfloat16)
    channel_in = rms_rows(residual, feedforward_norm_gain)
    upward = jnp.maximum(jnp.dot(channel_in, up_projection_weight, preferred_element_type=jnp.float32), 0.0)
    squared = (upward * upward).astype(jnp.bfloat16)
    return (residual.astype(jnp.float32) + split_sum(squared, down_projection_weight)).astype(jnp.bfloat16)
```

```python
import jax
import jax.numpy as jnp
from jax import lax
from jax.sharding import PartitionSpec as P

RUN = 4
PIECE_LIMIT = 1 << 20


def from_everyone(x, axis):
    copies = jnp.broadcast_to(x, (lax.axis_size(axis), *x.shape))
    return lax.all_to_all(copies, axis, split_axis=0, concat_axis=0, tiled=True)


def laid_out(tiles, dim):
    tiles = jnp.moveaxis(tiles, 0, dim)
    lengths = tiles.shape
    return tiles.reshape(*lengths[:dim], lengths[dim] * lengths[dim + 1], *lengths[dim + 2 :])


def collect(x, axis, dim):
    tiles = from_everyone(x, axis)
    return laid_out(tiles, dim)


def in_blocks(x, dim, peers):
    lengths = x.shape
    tiles = x.reshape(*lengths[:dim], peers, lengths[dim] // peers, *lengths[dim + 1 :])
    return jnp.moveaxis(tiles, dim, 0)


def sent_and_summed(x, axis, dim):
    peers = lax.axis_size(axis)
    tiles = lax.all_to_all(in_blocks(x, dim, peers), axis, 0, 0, tiled=True)
    return jnp.sum(tiles.astype(jnp.float32), axis=0)


def parts_of_all_groups(mine):
    groups = lax.axis_size("grp")
    me = lax.axis_index("grp")
    up = [(k, (k + 1) % groups) for k in range(groups)]
    down = [(k, (k - 1) % groups) for k in range(groups)]
    behind = [mine]
    ahead = []
    for _ in range(groups // 2):
        behind.append(lax.ppermute(behind[-1], "grp", up))
    for _ in range((groups - 1) // 2):
        ahead.append(lax.ppermute(ahead[-1] if ahead else mine, "grp", down))
    relative = behind + ahead[::-1]
    if groups == 1:
        return relative
    if groups == 2:
        first = me == 0
        return [
            jnp.where(first, relative[0], relative[1]),
            jnp.where(first, relative[1], relative[0]),
        ]
    stacked = jnp.stack(relative)
    return [
        lax.dynamic_index_in_dim(stacked, (me - k) % groups, 0, keepdims=False)
        for k in range(groups)
    ]


def gather_early(shard):
    rows, cols = shard.shape
    groups = lax.axis_size("grp")
    me = lax.axis_index("grp")
    ring = lax.axis_size("fs")
    runs = ring // RUN
    part = lax.dynamic_slice_in_dim(shard, me * (rows // groups), rows // groups, 0)
    strided = [[k + RUN * j for j in range(runs)] for k in range(RUN)]
    close = [[RUN * m + k for k in range(RUN)] for m in range(runs)]
    level = lax.all_gather(part, "fs", axis=0, tiled=True, axis_index_groups=strided)
    total = ring * (rows // groups) * cols * 2
    pieces = 1
    while total // pieces >= PIECE_LIMIT:
        pieces += 1
    wide = cols // pieces
    done = []
    for k in range(pieces):
        got = lax.all_gather(
            level[:, k * wide : (k + 1) * wide],
            "fs",
            axis=0,
            tiled=True,
            axis_index_groups=close,
        )
        done.append(parts_of_all_groups(got))
    whole = []
    for got in done:
        tiles = jnp.stack([p.reshape(RUN, runs, rows // groups, -1) for p in got], axis=2)
        whole.append(jnp.moveaxis(tiles, 1, 0).reshape(ring * rows, -1))
    return jnp.concatenate(whole, axis=1)


def rms_rows(values_in, norm_gain):
    values = values_in.astype(jnp.float32)
    inverse = lax.rsqrt(jnp.mean(values * values, axis=-1, keepdims=True) + 1e-06)
    return (values * inverse * norm_gain).astype(jnp.bfloat16)


def combine(earlier, later):
    return (earlier[0] * later[0], later[0] * earlier[1] + later[1])


def recurrent_state(
    recurrent_branch_rows,
    gate_branch_rows,
    convolution_kernel,
    decay_gate_matrix,
    input_gate_matrix,
    base_decay_logit,
    extra_log_decay,
):
    length = recurrent_branch_rows.shape[0]
    taps = convolution_kernel.shape[0]
    padded = jnp.pad(recurrent_branch_rows.astype(jnp.float32), ((taps - 1, 0), (0, 0)))
    conv_sum = jnp.zeros((length, recurrent_branch_rows.shape[1]), jnp.float32)
    for tap_index in range(taps):
        conv_sum = conv_sum + padded[tap_index : tap_index + length] * convolution_kernel[
            tap_index
        ].astype(jnp.float32)
    conv_rows = conv_sum.astype(jnp.bfloat16)
    blocks = decay_gate_matrix.shape[0]
    blocked = conv_rows.reshape(length, blocks, -1)
    recurrence_gate = jax.nn.sigmoid(
        jnp.einsum(
            "tni,nij->tnj", blocked, decay_gate_matrix, preferred_element_type=jnp.float32
        ).reshape(length, -1)
    )
    input_rate = jax.nn.sigmoid(
        jnp.einsum(
            "tni,nij->tnj", blocked, input_gate_matrix, preferred_element_type=jnp.float32
        ).reshape(length, -1)
    )
    decay_log_values = (
        -8.0 * jax.nn.softplus(-base_decay_logit) * recurrence_gate + extra_log_decay[:, None]
    )
    decay = jnp.exp(decay_log_values)
    drive = (
        jnp.sqrt(-jnp.expm1(2.0 * decay_log_values)) * input_rate * conv_rows.astype(jnp.float32)
    )
    _, hidden = lax.associative_scan(combine, (decay, drive), axis=0)
    return (hidden * gate_branch_rows.astype(jnp.float32)).astype(jnp.bfloat16)


def per_device(
    tokens,
    recurrent_norm_gain,
    feedforward_norm_gain,
    gate_projection_weight,
    recurrent_projection_weight,
    convolution_kernel,
    decay_gate_matrix,
    input_gate_matrix,
    base_decay_logit,
    extra_log_decay,
    output_projection_weight,
    up_projection_weight,
    down_projection_weight,
):
    late = jnp.concatenate([up_projection_weight, down_projection_weight.T], axis=1)
    late, gate_shard, tokens = lax.optimization_barrier((late, gate_projection_weight, tokens))
    late_whole = lax.all_gather(late, "fs", axis=0, tiled=True)
    whole_rows = collect(tokens, "tp", 1)
    early = jnp.concatenate(
        [gate_shard, recurrent_projection_weight, output_projection_weight.T], axis=1
    )
    early_whole = gather_early(early)
    width = gate_projection_weight.shape[1]
    gate_whole = early_whole[:, :width]
    recur_whole = early_whole[:, width : 2 * width]
    out_whole = early_whole[:, 2 * width :].T
    normed = rms_rows(whole_rows, recurrent_norm_gain)
    gate_pre = jnp.dot(normed, gate_whole, preferred_element_type=jnp.float32)
    recur_pre = jnp.dot(normed, recur_whole, preferred_element_type=jnp.float32)
    gate_branch_rows = jax.nn.gelu(gate_pre).astype(jnp.bfloat16)
    recurrent_branch_rows = recur_pre.astype(jnp.bfloat16)
    mixed_output = recurrent_state(
        recurrent_branch_rows,
        gate_branch_rows,
        convolution_kernel,
        decay_gate_matrix,
        input_gate_matrix,
        base_decay_logit,
        extra_log_decay,
    )
    partials = jnp.dot(mixed_output, out_whole, preferred_element_type=jnp.float32)
    residual = (
        tokens.astype(jnp.float32) + sent_and_summed(partials.astype(jnp.bfloat16), "tp", 1)
    ).astype(jnp.bfloat16)
    middle = collect(residual, "tp", 1)
    channel_in = rms_rows(middle, feedforward_norm_gain)
    hidden_width = up_projection_weight.shape[1]
    upward = jnp.dot(
        channel_in, late_whole[:, :hidden_width], preferred_element_type=jnp.float32
    )
    positive = jnp.maximum(upward, 0.0)
    squared = (positive * positive).astype(jnp.bfloat16)
    down_terms = jnp.dot(
        squared, late_whole[:, hidden_width:].T, preferred_element_type=jnp.float32
    )
    summed_down = sent_and_summed(down_terms.astype(jnp.bfloat16), "tp", 1)
    return (residual.astype(jnp.float32) + summed_down).astype(jnp.bfloat16)


def solution(mesh):
    placed = (
        P(("grp", "fs"), "tp"),
        P(),
        P(),
        P("fs", "tp"),
        P("fs", "tp"),
        P(None, "tp"),
        P("tp", None, None),
        P("tp", None, None),
        P("tp"),
        P(("grp", "fs")),
        P("tp", "fs"),
        P("fs", "tp"),
        P("tp", "fs"),
    )
    return jax.shard_map(
        per_device, mesh=mesh, in_specs=placed, out_specs=P(("grp", "fs"), "tp"), check_vma=False
    )
```

```python
import jax
import jax.numpy as jnp
from jax import lax
from jax.experimental import pallas as pl
from jax.experimental.pallas import tpu as pltpu
from jax.sharding import PartitionSpec as P

RUN = 4
PIECE_LIMIT = 1 << 20


def from_everyone(x, axis):
    copies = jnp.broadcast_to(x, (lax.axis_size(axis), *x.shape))
    return lax.all_to_all(copies, axis, split_axis=0, concat_axis=0, tiled=True)


def laid_out(tiles, dim):
    tiles = jnp.moveaxis(tiles, 0, dim)
    lengths = tiles.shape
    return tiles.reshape(*lengths[:dim], lengths[dim] * lengths[dim + 1], *lengths[dim + 2 :])


def collect(x, axis, dim):
    tiles = from_everyone(x, axis)
    return laid_out(tiles, dim)


def in_blocks(x, dim, peers):
    lengths = x.shape
    tiles = x.reshape(*lengths[:dim], peers, lengths[dim] // peers, *lengths[dim + 1 :])
    return jnp.moveaxis(tiles, dim, 0)


def sent_and_summed(x, axis, dim):
    peers = lax.axis_size(axis)
    tiles = lax.all_to_all(in_blocks(x, dim, peers), axis, 0, 0, tiled=True)
    return jnp.sum(tiles.astype(jnp.float32), axis=0)


def parts_of_all_groups(mine):
    groups = lax.axis_size("grp")
    up = [(k, (k + 1) % groups) for k in range(groups)]
    down = [(k, (k - 1) % groups) for k in range(groups)]
    behind = [mine]
    ahead = []
    for _ in range(groups // 2):
        behind.append(lax.ppermute(behind[-1], "grp", up))
    for _ in range((groups - 1) // 2):
        ahead.append(lax.ppermute(ahead[-1] if ahead else mine, "grp", down))
    return behind + ahead[::-1]


def gather_early(shard):
    rows, cols = shard.shape
    groups = lax.axis_size("grp")
    me = lax.axis_index("grp")
    ring = lax.axis_size("fs")
    runs = ring // RUN
    part = lax.dynamic_slice_in_dim(shard, me * (rows // groups), rows // groups, 0)
    strided = [[k + RUN * j for j in range(runs)] for k in range(RUN)]
    close = [[RUN * m + k for k in range(RUN)] for m in range(runs)]
    level = lax.all_gather(part, "fs", axis=0, tiled=True, axis_index_groups=strided)
    total = ring * (rows // groups) * cols * 2
    pieces = 1
    while total // pieces >= PIECE_LIMIT:
        pieces += 1
    wide = cols // pieces
    done = []
    for k in range(pieces):
        got = lax.all_gather(
            level[:, k * wide : (k + 1) * wide],
            "fs",
            axis=0,
            tiled=True,
            axis_index_groups=close,
        )
        done.append(parts_of_all_groups(got))
    return done


def rms_rows(values_in, norm_gain):
    values = values_in.astype(jnp.float32)
    inverse = lax.rsqrt(jnp.mean(values * values, axis=-1, keepdims=True) + 1e-06)
    return (values * inverse * norm_gain).astype(jnp.bfloat16)


def shifted(x, by, fill):
    rows = lax.broadcasted_iota(jnp.int32, x.shape, 0)
    return jnp.where(rows >= by, pltpu.roll(x, by, 0), fill)


def recurrent_body(groups, pieces, runs, me_ref, *refs):
    parts = refs[: pieces * groups]
    (tiles, gain, taps, decay_gate, input_gate, rate, extra, out, normed, weights) = refs[
        pieces * groups :
    ]
    blocks, length, block = tiles.shape
    width = taps.shape[1]
    each = parts[0].shape[0] // (RUN * runs)
    wide = parts[0].shape[1]
    for behind in range(groups):
        place = lax.rem(me_ref[0] + groups - behind, groups) * each
        for near in range(RUN):
            for far in range(runs):
                to = pl.multiple_of((far * RUN + near) * groups * each + place, each)
                start = (near * runs + far) * each
                for piece in range(pieces):
                    weights[pl.ds(to, each), piece * wide : (piece + 1) * wide] = parts[
                        piece * groups + behind
                    ][start : start + each, :]
    squares = jnp.zeros((length, 1), jnp.float32)
    for k in range(blocks):
        v = tiles[k].astype(jnp.float32)
        squares = squares + jnp.sum(v * v, axis=-1, keepdims=True)
    inverse = lax.rsqrt(squares / (blocks * block) + 1e-06)
    for k in range(blocks):
        here = slice(k * block, (k + 1) * block)
        normed[:, here] = (tiles[k].astype(jnp.float32) * inverse * gain[:, here]).astype(
            jnp.bfloat16
        )
    recur = jnp.dot(normed[...], weights[:, :width], preferred_element_type=jnp.float32)
    gate_pre = jnp.dot(
        normed[...], weights[:, width : 2 * width], preferred_element_type=jnp.float32
    )
    gate = jax.nn.gelu(gate_pre).astype(jnp.bfloat16).astype(jnp.float32)
    recur = recur.astype(jnp.bfloat16).astype(jnp.float32)
    count = taps.shape[0]
    conv_sum = recur * taps[count - 1 : count, :].astype(jnp.float32)
    for k in range(1, count):
        conv_sum = conv_sum + shifted(recur, k, 0.0) * taps[count - 1 - k : count - k, :].astype(
            jnp.float32
        )
    conv_rows = conv_sum.astype(jnp.bfloat16)
    maps = decay_gate.shape[0]
    size = width // maps
    recur_gate = []
    input_rate = []
    for k in range(maps):
        x = conv_rows[:, k * size : (k + 1) * size]
        recur_gate.append(jnp.dot(x, decay_gate[k], preferred_element_type=jnp.float32))
        input_rate.append(jnp.dot(x, input_gate[k], preferred_element_type=jnp.float32))
    recur_gate = jax.nn.sigmoid(jnp.concatenate(recur_gate, axis=1))
    input_rate = jax.nn.sigmoid(jnp.concatenate(input_rate, axis=1))
    log_decay = rate[...] * recur_gate + extra[...]
    decay = jnp.exp(log_decay)
    u = -log_decay
    small = 2.0 * u * (1.0 - u * (1.0 - u * (2.0 / 3.0 - u * (1.0 / 3.0 - u * (2.0 / 15.0)))))
    lost = jnp.where(u < 0.015625, small, 1.0 - decay * decay)
    hidden = jnp.sqrt(lost) * input_rate * conv_rows.astype(jnp.float32)
    by = 1
    while by < length:
        hidden = hidden + decay * shifted(hidden, by, 0.0)
        if 2 * by < length:
            decay = decay * shifted(decay, by, 1.0)
        by *= 2
    mixed = (hidden * gate).astype(jnp.bfloat16)
    for k in range(blocks):
        out[k] = lax.dot_general(
            mixed,
            weights[k * block : (k + 1) * block, 2 * width : 3 * width],
            (((1,), (1,)), ((), ())),
            preferred_element_type=jnp.float32,
        ).astype(jnp.bfloat16)


def recurrent_block(tiles, parts, gain, taps, decay_gate, input_gate, base, extra):
    groups = len(parts[0])
    pieces = len(parts)
    runs = lax.axis_size("fs") // RUN
    me = lax.axis_index("grp")
    rate = (-8.0 * jax.nn.softplus(-base))[None, :]
    flat = [p for piece in parts for p in piece]
    blocks, length, block = tiles.shape
    vmem = pl.BlockSpec(memory_space=pltpu.VMEM)
    features = blocks * block
    cols = pieces * parts[0][0].shape[1]
    return pl.pallas_call(
        lambda *refs: recurrent_body(groups, pieces, runs, *refs),
        out_shape=jax.ShapeDtypeStruct(tiles.shape, jnp.bfloat16),
        in_specs=[pl.BlockSpec(memory_space=pltpu.SMEM)] + [vmem] * (len(flat) + 7),
        out_specs=vmem,
        scratch_shapes=[
            pltpu.VMEM((length, features), jnp.bfloat16),
            pltpu.VMEM((features, cols), jnp.bfloat16),
        ],
        cost_estimate=pl.CostEstimate(
            flops=2 * length * features * cols,
            transcendentals=6 * length * taps.shape[1],
            bytes_accessed=2 * (features * cols + 2 * length * features),
        ),
        compiler_params=pltpu.CompilerParams(vmem_limit_bytes=40 << 20),
        name="recurrent",
    )(
        jnp.full((1,), me, jnp.int32),
        *flat,
        tiles,
        gain[None, :],
        taps,
        decay_gate,
        input_gate,
        rate,
        extra[:, None],
    )


def per_device(
    tokens,
    recurrent_norm_gain,
    feedforward_norm_gain,
    gate_projection_weight,
    recurrent_projection_weight,
    convolution_kernel,
    decay_gate_matrix,
    input_gate_matrix,
    base_decay_logit,
    extra_log_decay,
    output_projection_weight,
    up_projection_weight,
    down_projection_weight,
):
    late = jnp.concatenate([up_projection_weight, down_projection_weight.T], axis=1)
    late, tokens = lax.optimization_barrier((late, tokens))
    late_whole = lax.all_gather(late, "fs", axis=0, tiled=True)
    token_tiles = from_everyone(tokens, "tp")
    early = jnp.concatenate(
        [recurrent_projection_weight, gate_projection_weight, output_projection_weight.T], axis=1
    )
    partials = recurrent_block(
        token_tiles,
        gather_early(early),
        recurrent_norm_gain,
        convolution_kernel,
        decay_gate_matrix,
        input_gate_matrix,
        base_decay_logit,
        extra_log_decay,
    )
    arrived = lax.all_to_all(partials, "tp", 0, 0, tiled=True)
    residual = (
        tokens.astype(jnp.float32) + jnp.sum(arrived.astype(jnp.float32), axis=0)
    ).astype(jnp.bfloat16)
    middle = collect(residual, "tp", 1)
    channel_in = rms_rows(middle, feedforward_norm_gain)
    hidden_width = up_projection_weight.shape[1]
    upward = jnp.dot(
        channel_in, late_whole[:, :hidden_width], preferred_element_type=jnp.float32
    )
    positive = jnp.maximum(upward, 0.0)
    squared = (positive * positive).astype(jnp.bfloat16)
    down_terms = jnp.dot(
        squared, late_whole[:, hidden_width:].T, preferred_element_type=jnp.float32
    )
    summed_down = sent_and_summed(down_terms.astype(jnp.bfloat16), "tp", 1)
    return (residual.astype(jnp.float32) + summed_down).astype(jnp.bfloat16)


def solution(mesh):
    placed = (
        P(("grp", "fs"), "tp"),
        P(),
        P(),
        P("fs", "tp"),
        P("fs", "tp"),
        P(None, "tp"),
        P("tp", None, None),
        P("tp", None, None),
        P("tp"),
        P(("grp", "fs")),
        P("tp", "fs"),
        P("fs", "tp"),
        P("tp", "fs"),
    )
    return jax.shard_map(
        per_device, mesh=mesh, in_specs=placed, out_specs=P(("grp", "fs"), "tp"), check_vma=False
    )
```

```python
import jax
import jax.numpy as jnp
from jax import lax
from jax.experimental import pallas as pl
from jax.experimental.pallas import tpu as pltpu
from jax.sharding import PartitionSpec as P


RUN = 4
CHUNK = 256
PIECES = 2


def from_everyone(x, axis):
    copies = jnp.broadcast_to(x, (lax.axis_size(axis), *x.shape))
    return lax.all_to_all(copies, axis, split_axis=0, concat_axis=0, tiled=True)


def parts_of_all_groups(mine):
    groups = lax.axis_size("grp")
    up = [(k, (k + 1) % groups) for k in range(groups)]
    down = [(k, (k - 1) % groups) for k in range(groups)]
    behind = [mine]
    ahead = []
    for _ in range(groups // 2):
        behind.append(lax.ppermute(behind[-1], "grp", up))
    for _ in range((groups - 1) // 2):
        ahead.append(lax.ppermute(ahead[-1] if ahead else mine, "grp", down))
    return behind + ahead[::-1]


def gather_early(shard, waiting):
    rows, cols = shard.shape
    groups = lax.axis_size("grp")
    me = lax.axis_index("grp")
    ring = lax.axis_size("fs")
    runs = ring // RUN
    part = lax.dynamic_slice_in_dim(shard, me * (rows // groups), rows // groups, 0)
    strided = [[k + RUN * j for j in range(runs)] for k in range(RUN)]
    close = [[RUN * m + k for k in range(RUN)] for m in range(runs)]
    level = lax.all_gather(part, "fs", axis=0, tiled=True, axis_index_groups=strided)
    pieces = PIECES
    wide = cols // pieces
    done = []
    for k in range(pieces):
        piece = level[:, k * wide : (k + 1) * wide]
        got = lax.all_to_all(
            jnp.broadcast_to(piece, (RUN, *piece.shape)),
            "fs",
            0,
            0,
            tiled=True,
            axis_index_groups=close,
        ).reshape(-1, wide)
        if k == pieces - 1:
            got, waiting = lax.optimization_barrier((got, waiting))
        done.append(parts_of_all_groups(got))
    return done, waiting


def shifted(x, by, fill):
    rows = lax.broadcasted_iota(jnp.int32, x.shape, 0)
    return jnp.where(rows >= by, pltpu.roll(x, by, 0), fill)


def recurrent_body(groups, pieces, runs, me_ref, *refs):
    parts = refs[: pieces * groups]
    (tiles, gain, taps, maps, rate, extra, out, normed, weights) = refs[
        pieces * groups :
    ]
    blocks, length, block = tiles.shape
    width = taps.shape[1]
    each = parts[0].shape[0] // (RUN * runs)
    wide = parts[0].shape[1]
    for behind in range(groups):
        place = lax.rem(me_ref[0] + groups - behind, groups) * each
        for near in range(RUN):
            for far in range(runs):
                to = pl.multiple_of((far * RUN + near) * groups * each + place, each)
                start = (near * runs + far) * each
                for piece in range(pieces):
                    weights[pl.ds(to, each), piece * wide : (piece + 1) * wide] = parts[
                        piece * groups + behind
                    ][start : start + each, :]
    squares = jnp.zeros((length, 1), jnp.float32)
    for k in range(blocks):
        v = tiles[k].astype(jnp.float32)
        squares = squares + jnp.sum(v * v, axis=-1, keepdims=True)
    inverse = lax.rsqrt(squares / (blocks * block) + 1e-06)
    for k in range(blocks):
        here = slice(k * block, (k + 1) * block)
        normed[:, here] = (tiles[k].astype(jnp.float32) * inverse * gain[:, here]).astype(
            jnp.bfloat16
        )
    recur = jnp.dot(normed[...], weights[:, :width], preferred_element_type=jnp.float32)
    gate_pre = jnp.dot(
        normed[...], weights[:, width : 2 * width], preferred_element_type=jnp.float32
    )
    gate = jax.nn.gelu(gate_pre).astype(jnp.bfloat16).astype(jnp.float32)
    recur = recur.astype(jnp.bfloat16).astype(jnp.float32)
    count = taps.shape[0]
    conv_sum = recur * taps[count - 1 : count, :].astype(jnp.float32)
    for k in range(1, count):
        conv_sum = conv_sum + shifted(recur, k, 0.0) * taps[count - 1 - k : count - k, :].astype(
            jnp.float32
        )
    conv_rows = conv_sum.astype(jnp.bfloat16)
    count = maps.shape[0] // 2
    size = width // count
    recur_gate = []
    input_rate = []
    for k in range(count):
        x = conv_rows[:, k * size : (k + 1) * size]
        recur_gate.append(jnp.dot(x, maps[k], preferred_element_type=jnp.float32))
        input_rate.append(jnp.dot(x, maps[count + k], preferred_element_type=jnp.float32))
    recur_gate = jax.nn.sigmoid(jnp.concatenate(recur_gate, axis=1))
    input_rate = jax.nn.sigmoid(jnp.concatenate(input_rate, axis=1))
    log_decay = rate[...] * recur_gate + extra[...]
    decay = jnp.exp(log_decay)
    u = -log_decay
    small = 2.0 * u * (1.0 - u * (1.0 - u * (2.0 / 3.0 - u * (1.0 / 3.0 - u * (2.0 / 15.0)))))
    lost = jnp.where(u < 0.015625, small, 1.0 - decay * decay)
    hidden = jnp.sqrt(lost) * input_rate * conv_rows.astype(jnp.float32)
    by = 1
    while by < length:
        hidden = hidden + decay * shifted(hidden, by, 0.0)
        if 2 * by < length:
            decay = decay * shifted(decay, by, 1.0)
        by *= 2
    mixed = (hidden * gate).astype(jnp.bfloat16)
    for k in range(blocks):
        out[k] = lax.dot_general(
            mixed,
            weights[k * block : (k + 1) * block, 2 * width : 3 * width],
            (((1,), (1,)), ((), ())),
            preferred_element_type=jnp.float32,
        ).astype(jnp.bfloat16)


def recurrent_block(tiles, parts, gain, taps, decay_gate, input_gate, base, extra):
    groups = len(parts[0])
    pieces = len(parts)
    runs = lax.axis_size("fs") // RUN
    me = lax.axis_index("grp")
    rate = (-8.0 * jax.nn.softplus(-base))[None, :]
    flat = [p for piece in parts for p in piece]
    blocks, length, block = tiles.shape
    vmem = pl.BlockSpec(memory_space=pltpu.VMEM)
    features = blocks * block
    cols = pieces * parts[0][0].shape[1]
    return pl.pallas_call(
        lambda *refs: recurrent_body(groups, pieces, runs, *refs),
        out_shape=jax.ShapeDtypeStruct(tiles.shape, jnp.bfloat16),
        in_specs=[pl.BlockSpec(memory_space=pltpu.SMEM)] + [vmem] * (len(flat) + 6),
        out_specs=vmem,
        scratch_shapes=[
            pltpu.VMEM((length, features), jnp.bfloat16),
            pltpu.VMEM((features, cols), jnp.bfloat16),
        ],
        cost_estimate=pl.CostEstimate(
            flops=2 * length * features * cols,
            transcendentals=6 * length * taps.shape[1],
            bytes_accessed=2 * (features * cols + 2 * length * features),
        ),
        compiler_params=pltpu.CompilerParams(vmem_limit_bytes=40 << 20),
        name="recurrent",
    )(
        jnp.full((1,), me, jnp.int32),
        *flat,
        tiles,
        gain[None, :],
        taps,
        jnp.concatenate([decay_gate, input_gate]),
        rate,
        extra[:, None],
    )


def feed_forward_body(tiles, gain, weights, out, normed, total, held, arrived):
    blocks, length, block = tiles.shape
    steps = held.shape[0] // 2
    copies = [
        pltpu.make_async_copy(
            weights.at[:, k * CHUNK : (k + 1) * CHUNK], held.at[k], arrived.at[k]
        )
        for k in range(2 * steps)
    ]
    for k in range(steps):
        copies[k].start()
        copies[steps + k].start()
    squares = jnp.zeros((length, 1), jnp.float32)
    for k in range(blocks):
        v = tiles[k].astype(jnp.float32)
        squares = squares + jnp.sum(v * v, axis=-1, keepdims=True)
    inverse = lax.rsqrt(squares / (blocks * block) + 1e-06)
    for k in range(blocks):
        here = slice(k * block, (k + 1) * block)
        normed[:, here] = (tiles[k].astype(jnp.float32) * inverse * gain[:, here]).astype(
            jnp.bfloat16
        )
    for step in range(steps):
        copies[step].wait()
        upward = jnp.dot(normed[...], held[step], preferred_element_type=jnp.float32)
        positive = jnp.maximum(upward, 0.0)
        squared = (positive * positive).astype(jnp.bfloat16)
        copies[steps + step].wait()
        for k in range(blocks):
            product = lax.dot_general(
                squared,
                held[steps + step, k * block : (k + 1) * block, :],
                (((1,), (1,)), ((), ())),
                preferred_element_type=jnp.float32,
            )
            product = product if step == 0 else total[k] + product
            if step < steps - 1:
                total[k] = product
            else:
                out[k] = product.astype(jnp.bfloat16)


def feed_forward(tiles, gain, weights):
    _, length, _ = tiles.shape
    features, both = weights.shape
    vmem = pl.BlockSpec(memory_space=pltpu.VMEM)
    return pl.pallas_call(
        feed_forward_body,
        out_shape=jax.ShapeDtypeStruct(tiles.shape, jnp.bfloat16),
        in_specs=[vmem, vmem, pl.BlockSpec(memory_space=pltpu.HBM)],
        out_specs=vmem,
        scratch_shapes=[
            pltpu.VMEM((length, features), jnp.bfloat16),
            pltpu.VMEM(tiles.shape, jnp.float32),
            pltpu.VMEM((both // CHUNK, features, CHUNK), jnp.bfloat16),
            pltpu.SemaphoreType.DMA((both // CHUNK,)),
        ],
        cost_estimate=pl.CostEstimate(
            flops=2 * length * features * both,
            transcendentals=length,
            bytes_accessed=2 * (features * both + 2 * length * features),
        ),
        compiler_params=pltpu.CompilerParams(vmem_limit_bytes=40 << 20),
        name="feed_forward",
    )(tiles, gain[None, :], pltpu.with_memory_space_constraint(weights, pltpu.HBM))


def per_device(
    tokens,
    recurrent_norm_gain,
    feedforward_norm_gain,
    gate_projection_weight,
    recurrent_projection_weight,
    convolution_kernel,
    decay_gate_matrix,
    input_gate_matrix,
    base_decay_logit,
    extra_log_decay,
    output_projection_weight,
    up_projection_weight,
    down_projection_weight,
):
    late = jnp.concatenate([up_projection_weight, down_projection_weight.T], axis=1)
    late, tokens = lax.optimization_barrier((late, tokens))
    late_whole = lax.all_gather(late, "fs", axis=0, tiled=True)
    early = jnp.concatenate(
        [recurrent_projection_weight, gate_projection_weight, output_projection_weight.T], axis=1
    )
    parts, held = gather_early(early, tokens)
    token_tiles = from_everyone(held, "tp")
    partials = recurrent_block(
        token_tiles,
        parts,
        recurrent_norm_gain,
        convolution_kernel,
        decay_gate_matrix,
        input_gate_matrix,
        base_decay_logit,
        extra_log_decay,
    )
    arrived = lax.all_to_all(partials, "tp", 0, 0, tiled=True)
    residual = (
        tokens.astype(jnp.float32) + jnp.sum(arrived.astype(jnp.float32), axis=0)
    ).astype(jnp.bfloat16)
    down_terms = feed_forward(from_everyone(residual, "tp"), feedforward_norm_gain, late_whole)
    returned = lax.all_to_all(down_terms, "tp", 0, 0, tiled=True)
    return (
        residual.astype(jnp.float32) + jnp.sum(returned.astype(jnp.float32), axis=0)
    ).astype(jnp.bfloat16)


def solution(mesh):
    placed = (
        P(("grp", "fs"), "tp"),
        P(),
        P(),
        P("fs", "tp"),
        P("fs", "tp"),
        P(None, "tp"),
        P("tp", None, None),
        P("tp", None, None),
        P("tp"),
        P(("grp", "fs")),
        P("tp", "fs"),
        P("fs", "tp"),
        P("tp", "fs"),
    )

    return jax.shard_map(
        per_device, mesh=mesh, in_specs=placed, out_specs=P(("grp", "fs"), "tp"), check_vma=False
    )
```

```python
import jax
import jax.numpy as jnp
from jax import lax
from jax.experimental import pallas as pl
from jax.experimental.pallas import tpu as pltpu
from jax.sharding import PartitionSpec as P


RUN = 4
CORES = 2
CHUNK = 256
PIECES = 2


def same_core():
    members = lax.axis_size("tp")
    return [list(range(c, members, CORES)) for c in range(CORES)]


def with_partner(x):
    members = lax.axis_size("tp")
    return lax.ppermute(x, "tp", [(k, k + 1 - 2 * (k % CORES)) for k in range(members)])


def from_everyone(x):
    groups = same_core()
    copies = jnp.broadcast_to(x, (len(groups[0]), *x.shape))
    mine = lax.all_to_all(copies, "tp", 0, 0, tiled=True, axis_index_groups=groups)
    return mine, with_partner(mine)


def summed_over_peers(keep, give):
    pair = keep.astype(jnp.float32) + with_partner(give).astype(jnp.float32)
    tiles = lax.all_to_all(
        pair.astype(jnp.bfloat16), "tp", 0, 0, tiled=True, axis_index_groups=same_core()
    )
    return jnp.sum(tiles.astype(jnp.float32), axis=0)


def norm_rows(core, mine, other, gain, normed):
    half, length, block = mine.shape
    blocks = CORES * half

    def tile(k):
        first = mine[k // CORES].astype(jnp.float32)
        second = other[k // CORES].astype(jnp.float32)
        return jnp.where(core == k % CORES, first, second)

    squares = jnp.zeros((length, 1), jnp.float32)
    for k in range(blocks):
        v = tile(k)
        squares = squares + jnp.sum(v * v, axis=-1, keepdims=True)
    inverse = lax.rsqrt(squares / (blocks * block) + 1e-06)
    for k in range(blocks):
        here = slice(k * block, (k + 1) * block)
        normed[:, here] = (tile(k) * inverse * gain[:, here]).astype(jnp.bfloat16)


def put(core, k, value, keep, give):
    @pl.when(core == k % CORES)
    def _():
        keep[k // CORES] = value

    @pl.when(core != k % CORES)
    def _():
        give[k // CORES] = value


def parts_of_all_groups(mine):
    groups = lax.axis_size("grp")
    up = [(k, (k + 1) % groups) for k in range(groups)]
    down = [(k, (k - 1) % groups) for k in range(groups)]
    behind = [mine]
    ahead = []
    for _ in range(groups // 2):
        behind.append(lax.ppermute(behind[-1], "grp", up))
    for _ in range((groups - 1) // 2):
        ahead.append(lax.ppermute(ahead[-1] if ahead else mine, "grp", down))
    return behind + ahead[::-1]


def gather_early(shard, waiting):
    rows, cols = shard.shape
    groups = lax.axis_size("grp")
    me = lax.axis_index("grp")
    ring = lax.axis_size("fs")
    runs = ring // RUN
    part = lax.dynamic_slice_in_dim(shard, me * (rows // groups), rows // groups, 0)
    strided = [[k + RUN * j for j in range(runs)] for k in range(RUN)]
    close = [[RUN * m + k for k in range(RUN)] for m in range(runs)]
    level = lax.all_gather(part, "fs", axis=0, tiled=True, axis_index_groups=strided)
    pieces = PIECES
    wide = cols // pieces
    done = []
    for k in range(pieces):
        piece = level[:, k * wide : (k + 1) * wide]
        got = lax.all_gather(piece, "fs", axis=0, tiled=True, axis_index_groups=close)
        if k == pieces - 1:
            got, waiting = lax.optimization_barrier((got, waiting))
        done.append(parts_of_all_groups(got))
    return done, waiting


def shifted(x, by, fill):
    rows = lax.broadcasted_iota(jnp.int32, x.shape, 0)
    return jnp.where(rows >= by, pltpu.roll(x, by, 0), fill)


def recurrent_body(groups, pieces, runs, me_ref, *refs):
    parts = refs[: pieces * groups]
    (mine, other, gain, taps, maps, rate, extra, keep, give, normed, weights) = refs[
        pieces * groups :
    ]
    half, length, block = mine.shape
    blocks = CORES * half
    core = me_ref[1]
    width = taps.shape[1]
    each = parts[0].shape[0] // (RUN * runs)
    wide = parts[0].shape[1]
    for behind in range(groups):
        place = lax.rem(me_ref[0] + groups - behind, groups) * each
        for near in range(RUN):
            for far in range(runs):
                to = pl.multiple_of((far * RUN + near) * groups * each + place, each)
                start = (near * runs + far) * each
                for piece in range(pieces):
                    weights[pl.ds(to, each), piece * wide : (piece + 1) * wide] = parts[
                        piece * groups + behind
                    ][start : start + each, :]
    norm_rows(core, mine, other, gain, normed)
    recur = jnp.dot(normed[...], weights[:, :width], preferred_element_type=jnp.float32)
    gate_pre = jnp.dot(
        normed[...], weights[:, width : 2 * width], preferred_element_type=jnp.float32
    )
    gate = jax.nn.gelu(gate_pre).astype(jnp.bfloat16).astype(jnp.float32)
    recur = recur.astype(jnp.bfloat16).astype(jnp.float32)
    count = taps.shape[0]
    conv_sum = recur * taps[count - 1 : count, :].astype(jnp.float32)
    for k in range(1, count):
        conv_sum = conv_sum + shifted(recur, k, 0.0) * taps[count - 1 - k : count - k, :].astype(
            jnp.float32
        )
    conv_rows = conv_sum.astype(jnp.bfloat16)
    count = maps.shape[0] // 2
    size = width // count
    recur_gate = []
    input_rate = []
    for k in range(count):
        x = conv_rows[:, k * size : (k + 1) * size]
        recur_gate.append(jnp.dot(x, maps[k], preferred_element_type=jnp.float32))
        input_rate.append(jnp.dot(x, maps[count + k], preferred_element_type=jnp.float32))
    recur_gate = jax.nn.sigmoid(jnp.concatenate(recur_gate, axis=1))
    input_rate = jax.nn.sigmoid(jnp.concatenate(input_rate, axis=1))
    log_decay = rate[...] * recur_gate + extra[...]
    decay = jnp.exp(log_decay)
    u = -log_decay
    small = 2.0 * u * (1.0 - u * (1.0 - u * (2.0 / 3.0 - u * (1.0 / 3.0 - u * (2.0 / 15.0)))))
    lost = jnp.where(u < 0.015625, small, 1.0 - decay * decay)
    hidden = jnp.sqrt(lost) * input_rate * conv_rows.astype(jnp.float32)
    by = 1
    while by < length:
        hidden = hidden + decay * shifted(hidden, by, 0.0)
        if 2 * by < length:
            decay = decay * shifted(decay, by, 1.0)
        by *= 2
    mixed = (hidden * gate).astype(jnp.bfloat16)
    for k in range(blocks):
        product = lax.dot_general(
            mixed,
            weights[k * block : (k + 1) * block, 2 * width : 3 * width],
            (((1,), (1,)), ((), ())),
            preferred_element_type=jnp.float32,
        )
        put(core, k, product.astype(jnp.bfloat16), keep, give)


def recurrent_block(tiles, parts, gain, taps, decay_gate, input_gate, base, extra):
    groups = len(parts[0])
    pieces = len(parts)
    runs = lax.axis_size("fs") // RUN
    place = jnp.stack([lax.axis_index("grp"), lax.axis_index("tp") % CORES]).astype(jnp.int32)
    rate = (-8.0 * jax.nn.softplus(-base))[None, :]
    flat = [p for piece in parts for p in piece]
    half, length, block = tiles[0].shape
    vmem = pl.BlockSpec(memory_space=pltpu.VMEM)
    features = CORES * half * block
    cols = pieces * parts[0][0].shape[1]
    return pl.pallas_call(
        lambda *refs: recurrent_body(groups, pieces, runs, *refs),
        out_shape=[jax.ShapeDtypeStruct(tiles[0].shape, jnp.bfloat16)] * 2,
        in_specs=[pl.BlockSpec(memory_space=pltpu.SMEM)] + [vmem] * (len(flat) + 7),
        out_specs=[vmem] * 2,
        scratch_shapes=[
            pltpu.VMEM((length, features), jnp.bfloat16),
            pltpu.VMEM((features, cols), jnp.bfloat16),
        ],
        cost_estimate=pl.CostEstimate(
            flops=2 * length * features * cols,
            transcendentals=6 * length * taps.shape[1],
            bytes_accessed=2 * (features * cols + 2 * length * features),
        ),
        compiler_params=pltpu.CompilerParams(vmem_limit_bytes=40 << 20),
        name="recurrent",
    )(
        place,
        *flat,
        *tiles,
        gain[None, :],
        taps,
        jnp.concatenate([decay_gate, input_gate]),
        rate,
        extra[:, None],
    )


def feed_forward_body(
    core_ref, mine, other, gain, weights, keep, give, normed, squared, up, down, arrived
):
    half, _, block = mine.shape
    blocks = CORES * half
    core = core_ref[0]
    hidden = squared.shape[1]
    chunks = hidden // CHUNK
    ups = [
        pltpu.make_async_copy(weights.at[:, k * CHUNK : (k + 1) * CHUNK], up.at[k], arrived.at[k])
        for k in range(chunks)
    ]
    downs = [
        pltpu.make_async_copy(
            weights.at[k * block : (k + 1) * block, hidden:], down.at[k], arrived.at[chunks + k]
        )
        for k in range(blocks)
    ]
    for copy in ups + downs:
        copy.start()
    norm_rows(core, mine, other, gain, normed)
    for k in range(chunks):
        ups[k].wait()
        upward = jnp.dot(normed[...], up[k], preferred_element_type=jnp.float32)
        positive = jnp.maximum(upward, 0.0)
        squared[:, k * CHUNK : (k + 1) * CHUNK] = (positive * positive).astype(jnp.bfloat16)
    for k in range(blocks):
        downs[k].wait()
        product = lax.dot_general(
            squared[...],
            down[k],
            (((1,), (1,)), ((), ())),
            preferred_element_type=jnp.float32,
        )
        put(core, k, product.astype(jnp.bfloat16), keep, give)


def feed_forward(tiles, gain, weights):
    _, length, block = tiles[0].shape
    features, both = weights.shape
    hidden = both // 2
    chunks = hidden // CHUNK
    vmem = pl.BlockSpec(memory_space=pltpu.VMEM)
    core = (lax.axis_index("tp") % CORES).astype(jnp.int32).reshape(1)
    return pl.pallas_call(
        feed_forward_body,
        out_shape=[jax.ShapeDtypeStruct(tiles[0].shape, jnp.bfloat16)] * 2,
        in_specs=[
            pl.BlockSpec(memory_space=pltpu.SMEM),
            vmem,
            vmem,
            vmem,
            pl.BlockSpec(memory_space=pltpu.HBM),
        ],
        out_specs=[vmem] * 2,
        scratch_shapes=[
            pltpu.VMEM((length, features), jnp.bfloat16),
            pltpu.VMEM((length, hidden), jnp.bfloat16),
            pltpu.VMEM((chunks, features, CHUNK), jnp.bfloat16),
            pltpu.VMEM((features // block, block, hidden), jnp.bfloat16),
            pltpu.SemaphoreType.DMA((chunks + features // block,)),
        ],
        cost_estimate=pl.CostEstimate(
            flops=2 * length * features * both,
            transcendentals=length,
            bytes_accessed=2 * (features * both + 2 * length * features),
        ),
        compiler_params=pltpu.CompilerParams(vmem_limit_bytes=40 << 20),
        name="feed_forward",
    )(core, *tiles, gain[None, :], pltpu.with_memory_space_constraint(weights, pltpu.HBM))


def per_device(
    tokens,
    recurrent_norm_gain,
    feedforward_norm_gain,
    gate_projection_weight,
    recurrent_projection_weight,
    convolution_kernel,
    decay_gate_matrix,
    input_gate_matrix,
    base_decay_logit,
    extra_log_decay,
    output_projection_weight,
    up_projection_weight,
    down_projection_weight,
):
    late = jnp.concatenate([up_projection_weight, down_projection_weight.T], axis=1)
    late, tokens = lax.optimization_barrier((late, tokens))
    late_whole = lax.all_gather(late, "fs", axis=0, tiled=True)
    early = jnp.concatenate(
        [recurrent_projection_weight, gate_projection_weight, output_projection_weight.T], axis=1
    )
    parts, held = gather_early(early, tokens)
    token_tiles = from_everyone(held)
    keep, give = recurrent_block(
        token_tiles,
        parts,
        recurrent_norm_gain,
        convolution_kernel,
        decay_gate_matrix,
        input_gate_matrix,
        base_decay_logit,
        extra_log_decay,
    )
    residual = (tokens.astype(jnp.float32) + summed_over_peers(keep, give)).astype(jnp.bfloat16)
    keep, give = feed_forward(from_everyone(residual), feedforward_norm_gain, late_whole)
    return (residual.astype(jnp.float32) + summed_over_peers(keep, give)).astype(jnp.bfloat16)


def solution(mesh):
    placed = (
        P(("grp", "fs"), "tp"),
        P(),
        P(),
        P("fs", "tp"),
        P("fs", "tp"),
        P(None, "tp"),
        P("tp", None, None),
        P("tp", None, None),
        P("tp"),
        P(("grp", "fs")),
        P("tp", "fs"),
        P("fs", "tp"),
        P("tp", "fs"),
    )

    return jax.shard_map(
        per_device, mesh=mesh, in_specs=placed, out_specs=P(("grp", "fs"), "tp"), check_vma=False
    )
```

```python
import jax
import jax.numpy as jnp
from jax import lax
from jax.experimental import pallas as pl
from jax.experimental.pallas import tpu as pltpu
from jax.sharding import PartitionSpec as P


RUN = 4
CORES = 2
CHUNK = 256
PIECES = 2


def same_core():
    members = lax.axis_size("tp")
    return [list(range(c, members, CORES)) for c in range(CORES)]


def with_partner(x):
    members = lax.axis_size("tp")
    return lax.ppermute(x, "tp", [(k, k + 1 - 2 * (k % CORES)) for k in range(members)])


def from_everyone(x):
    groups = same_core()
    copies = jnp.broadcast_to(x, (len(groups[0]), *x.shape))
    mine = lax.all_to_all(copies, "tp", 0, 0, tiled=True, axis_index_groups=groups)
    return mine, with_partner(mine)


def summed_over_peers(keep, give):
    pair = keep.astype(jnp.float32) + with_partner(give).astype(jnp.float32)
    tiles = lax.all_to_all(
        pair.astype(jnp.bfloat16), "tp", 0, 0, tiled=True, axis_index_groups=same_core()
    )
    return jnp.sum(tiles.astype(jnp.float32), axis=0)


def norm_rows(core, mine, other, gain, normed):
    half, length, block = mine.shape
    blocks = CORES * half

    def tile(k):
        return (mine if core == k % CORES else other)[k // CORES].astype(jnp.float32)

    squares = jnp.zeros((length, 1), jnp.float32)
    for k in range(blocks):
        v = tile(k)
        squares = squares + jnp.sum(v * v, axis=-1, keepdims=True)
    inverse = lax.rsqrt(squares / (blocks * block) + 1e-06)
    for k in range(blocks):
        here = slice(k * block, (k + 1) * block)
        normed[:, here] = (tile(k) * inverse * gain[:, here]).astype(jnp.bfloat16)


def put(core, k, value, keep, give):
    (keep if core == k % CORES else give)[k // CORES] = value


def on_each_core(core, body):
    for c in range(CORES):

        @pl.when(core == c)
        def _(c=c):
            body(c)


def parts_of_all_groups(mine):
    groups = lax.axis_size("grp")
    up = [(k, (k + 1) % groups) for k in range(groups)]
    down = [(k, (k - 1) % groups) for k in range(groups)]
    behind = [mine]
    ahead = []
    for _ in range(groups // 2):
        behind.append(lax.ppermute(behind[-1], "grp", up))
    for _ in range((groups - 1) // 2):
        ahead.append(lax.ppermute(ahead[-1] if ahead else mine, "grp", down))
    return behind + ahead[::-1]


def gather_early(shard, waiting):
    rows, cols = shard.shape
    groups = lax.axis_size("grp")
    me = lax.axis_index("grp")
    ring = lax.axis_size("fs")
    runs = ring // RUN
    part = lax.dynamic_slice_in_dim(shard, me * (rows // groups), rows // groups, 0)
    strided = [[k + RUN * j for j in range(runs)] for k in range(RUN)]
    close = [[RUN * m + k for k in range(RUN)] for m in range(runs)]
    level = lax.all_gather(part, "fs", axis=0, tiled=True, axis_index_groups=strided)
    pieces = PIECES
    wide = cols // pieces
    done = []
    for k in range(pieces):
        piece = level[:, k * wide : (k + 1) * wide]
        got = lax.all_gather(piece, "fs", axis=0, tiled=True, axis_index_groups=close)
        if k == pieces - 1:
            got, waiting = lax.optimization_barrier((got, waiting))
        done.append(parts_of_all_groups(got))
    return done, waiting


def shifted(x, by, fill):
    rows = lax.broadcasted_iota(jnp.int32, x.shape, 0)
    return jnp.where(rows >= by, pltpu.roll(x, by, 0), fill)


def recurrent_body(groups, pieces, runs, me_ref, *refs):
    parts = refs[: pieces * groups]
    mine, other, *small = refs[pieces * groups : pieces * groups + 8]
    keep, give, normed, weights, *held, landed = refs[pieces * groups + 8 :]
    copies = [pltpu.make_async_copy(s, h, landed.at[k]) for k, (s, h) in enumerate(zip(small, held))]
    for copy in copies:
        copy.start()
    gain, taps, decay_map, input_map, base, extra = held
    half, length, block = mine.shape
    blocks = CORES * half
    width = taps.shape[1]
    each = parts[0].shape[0] // (RUN * runs)
    wide = parts[0].shape[1]
    for behind in range(groups):
        place = lax.rem(me_ref[0] + groups - behind, groups) * each
        for near in range(RUN):
            for far in range(runs):
                to = pl.multiple_of((far * RUN + near) * groups * each + place, each)
                start = (near * runs + far) * each
                for piece in range(pieces):
                    weights[pl.ds(to, each), piece * wide : (piece + 1) * wide] = parts[
                        piece * groups + behind
                    ][start : start + each, :]
    for copy in copies:
        copy.wait()
    on_each_core(me_ref[1], lambda core: norm_rows(core, mine, other, gain, normed))
    recur = jnp.dot(normed[...], weights[:, :width], preferred_element_type=jnp.float32)
    gate_pre = jnp.dot(
        normed[...], weights[:, width : 2 * width], preferred_element_type=jnp.float32
    )
    gate = jax.nn.gelu(gate_pre).astype(jnp.bfloat16).astype(jnp.float32)
    recur = recur.astype(jnp.bfloat16).astype(jnp.float32)
    count = taps.shape[0]
    conv_sum = recur * taps[count - 1 : count, :].astype(jnp.float32)
    for k in range(1, count):
        conv_sum = conv_sum + shifted(recur, k, 0.0) * taps[count - 1 - k : count - k, :].astype(
            jnp.float32
        )
    conv_rows = conv_sum.astype(jnp.bfloat16)
    count = decay_map.shape[0]
    size = width // count
    recur_gate = []
    input_rate = []
    for k in range(count):
        x = conv_rows[:, k * size : (k + 1) * size]
        recur_gate.append(jnp.dot(x, decay_map[k], preferred_element_type=jnp.float32))
        input_rate.append(jnp.dot(x, input_map[k], preferred_element_type=jnp.float32))
    recur_gate = jax.nn.sigmoid(jnp.concatenate(recur_gate, axis=1))
    input_rate = jax.nn.sigmoid(jnp.concatenate(input_rate, axis=1))
    x = -base[...]
    softplus = jnp.maximum(x, 0.0) + jnp.log1p(jnp.exp(-jnp.abs(x)))
    columns = jnp.broadcast_to(extra[...], (128, length)).T
    columns = jnp.concatenate([columns] * (width // 128), axis=1)
    log_decay = -8.0 * softplus * recur_gate + columns
    decay = jnp.exp(log_decay)
    u = -log_decay
    small = 2.0 * u * (1.0 - u * (1.0 - u * (2.0 / 3.0 - u * (1.0 / 3.0 - u * (2.0 / 15.0)))))
    lost = jnp.where(u < 0.015625, small, 1.0 - decay * decay)
    hidden = jnp.sqrt(lost) * input_rate * conv_rows.astype(jnp.float32)
    by = 1
    while by < length:
        hidden = hidden + decay * shifted(hidden, by, 0.0)
        if 2 * by < length:
            decay = decay * shifted(decay, by, 1.0)
        by *= 2
    mixed = (hidden * gate).astype(jnp.bfloat16)

    def finish(core):
        for k in range(blocks):
            product = lax.dot_general(
                mixed,
                weights[k * block : (k + 1) * block, 2 * width : 3 * width],
                (((1,), (1,)), ((), ())),
                preferred_element_type=jnp.float32,
            )
            put(core, k, product.astype(jnp.bfloat16), keep, give)

    on_each_core(me_ref[1], finish)


def recurrent_block(tiles, parts, gain, taps, decay_gate, input_gate, base, extra):
    groups = len(parts[0])
    pieces = len(parts)
    runs = lax.axis_size("fs") // RUN
    place = jnp.stack([lax.axis_index("grp"), lax.axis_index("tp") % CORES]).astype(jnp.int32)
    small = [gain[None, :], taps, decay_gate, input_gate, base[None, :], extra[None, :]]
    flat = [p for piece in parts for p in piece]
    half, length, block = tiles[0].shape
    vmem = pl.BlockSpec(memory_space=pltpu.VMEM)
    features = CORES * half * block
    cols = pieces * parts[0][0].shape[1]
    return pl.pallas_call(
        lambda *refs: recurrent_body(groups, pieces, runs, *refs),
        out_shape=[jax.ShapeDtypeStruct(tiles[0].shape, jnp.bfloat16)] * 2,
        in_specs=[pl.BlockSpec(memory_space=pltpu.SMEM)] + [vmem] * (len(flat) + 2)
        + [pl.BlockSpec(memory_space=pltpu.HBM)] * len(small),
        out_specs=[vmem] * 2,
        scratch_shapes=[
            pltpu.VMEM((length, features), jnp.bfloat16),
            pltpu.VMEM((features, cols), jnp.bfloat16),
            *[pltpu.VMEM(s.shape, s.dtype) for s in small],
            pltpu.SemaphoreType.DMA((len(small),)),
        ],
        cost_estimate=pl.CostEstimate(
            flops=2 * length * features * cols,
            transcendentals=6 * length * taps.shape[1],
            bytes_accessed=2 * (features * cols + 2 * length * features),
        ),
        compiler_params=pltpu.CompilerParams(vmem_limit_bytes=40 << 20),
        name="recurrent",
    )(
        place,
        *flat,
        *tiles,
        *[pltpu.with_memory_space_constraint(s, pltpu.HBM) for s in small],
    )


def feed_forward_body(
    core_ref, mine, other, gain, weights, keep, give, normed, squared, up, down, arrived
):
    half, _, block = mine.shape
    blocks = CORES * half
    hidden = squared.shape[1]
    chunks = hidden // CHUNK
    ups = [
        pltpu.make_async_copy(weights.at[:, k * CHUNK : (k + 1) * CHUNK], up.at[k], arrived.at[k])
        for k in range(chunks)
    ]
    downs = [
        pltpu.make_async_copy(
            weights.at[k * block : (k + 1) * block, hidden:], down.at[k], arrived.at[chunks + k]
        )
        for k in range(blocks)
    ]
    for copy in ups + downs:
        copy.start()
    on_each_core(core_ref[0], lambda core: norm_rows(core, mine, other, gain, normed))
    for k in range(chunks):
        ups[k].wait()
        upward = jnp.dot(normed[...], up[k], preferred_element_type=jnp.float32)
        positive = jnp.maximum(upward, 0.0)
        squared[:, k * CHUNK : (k + 1) * CHUNK] = (positive * positive).astype(jnp.bfloat16)
    for copy in downs:
        copy.wait()

    def finish(core):
        for k in range(blocks):
            product = lax.dot_general(
                squared[...],
                down[k],
                (((1,), (1,)), ((), ())),
                preferred_element_type=jnp.float32,
            )
            put(core, k, product.astype(jnp.bfloat16), keep, give)

    on_each_core(core_ref[0], finish)


def feed_forward(tiles, gain, weights):
    _, length, block = tiles[0].shape
    features, both = weights.shape
    hidden = both // 2
    chunks = hidden // CHUNK
    vmem = pl.BlockSpec(memory_space=pltpu.VMEM)
    core = (lax.axis_index("tp") % CORES).astype(jnp.int32).reshape(1)
    return pl.pallas_call(
        feed_forward_body,
        out_shape=[jax.ShapeDtypeStruct(tiles[0].shape, jnp.bfloat16)] * 2,
        in_specs=[
            pl.BlockSpec(memory_space=pltpu.SMEM),
            vmem,
            vmem,
            vmem,
            pl.BlockSpec(memory_space=pltpu.HBM),
        ],
        out_specs=[vmem] * 2,
        scratch_shapes=[
            pltpu.VMEM((length, features), jnp.bfloat16),
            pltpu.VMEM((length, hidden), jnp.bfloat16),
            pltpu.VMEM((chunks, features, CHUNK), jnp.bfloat16),
            pltpu.VMEM((features // block, block, hidden), jnp.bfloat16),
            pltpu.SemaphoreType.DMA((chunks + features // block,)),
        ],
        cost_estimate=pl.CostEstimate(
            flops=2 * length * features * both,
            transcendentals=length,
            bytes_accessed=2 * (features * both + 2 * length * features),
        ),
        compiler_params=pltpu.CompilerParams(vmem_limit_bytes=40 << 20),
        name="feed_forward",
    )(core, *tiles, gain[None, :], pltpu.with_memory_space_constraint(weights, pltpu.HBM))


def per_device(
    tokens,
    recurrent_norm_gain,
    feedforward_norm_gain,
    gate_projection_weight,
    recurrent_projection_weight,
    convolution_kernel,
    decay_gate_matrix,
    input_gate_matrix,
    base_decay_logit,
    extra_log_decay,
    output_projection_weight,
    up_projection_weight,
    down_projection_weight,
):
    late = jnp.concatenate([up_projection_weight, down_projection_weight.T], axis=1)
    late, tokens = lax.optimization_barrier((late, tokens))
    late_whole = lax.all_gather(late, "fs", axis=0, tiled=True)
    early = jnp.concatenate(
        [recurrent_projection_weight, gate_projection_weight, output_projection_weight.T], axis=1
    )
    parts, held = gather_early(early, tokens)
    token_tiles = from_everyone(held)
    keep, give = recurrent_block(
        token_tiles,
        parts,
        recurrent_norm_gain,
        convolution_kernel,
        decay_gate_matrix,
        input_gate_matrix,
        base_decay_logit,
        extra_log_decay,
    )
    residual = (tokens.astype(jnp.float32) + summed_over_peers(keep, give)).astype(jnp.bfloat16)
    keep, give = feed_forward(from_everyone(residual), feedforward_norm_gain, late_whole)
    return (residual.astype(jnp.float32) + summed_over_peers(keep, give)).astype(jnp.bfloat16)


def solution(mesh):
    placed = (
        P(("grp", "fs"), "tp"),
        P(),
        P(),
        P("fs", "tp"),
        P("fs", "tp"),
        P(None, "tp"),
        P("tp", None, None),
        P("tp", None, None),
        P("tp"),
        P(("grp", "fs")),
        P("tp", "fs"),
        P("fs", "tp"),
        P("tp", "fs"),
    )

    return jax.shard_map(
        per_device, mesh=mesh, in_specs=placed, out_specs=P(("grp", "fs"), "tp"), check_vma=False
    )
```

```python
import jax
import jax.numpy as jnp
from jax import lax
from jax.experimental import pallas as pl
from jax.experimental.pallas import tpu as pltpu
from jax.sharding import PartitionSpec as P


RUN = 2
CORES = 2
CHUNK = 256
PIECES = 2


def same_core():
    members = lax.axis_size("tp")
    return [list(range(c, members, CORES)) for c in range(CORES)]


def with_partner(x):
    members = lax.axis_size("tp")
    return lax.ppermute(x, "tp", [(k, k + 1 - 2 * (k % CORES)) for k in range(members)])


def from_everyone(x):
    groups = same_core()
    copies = jnp.broadcast_to(x, (len(groups[0]), *x.shape))
    mine = lax.all_to_all(copies, "tp", 0, 0, tiled=True, axis_index_groups=groups)
    return mine, with_partner(mine)


def summed_over_peers(keep, give):
    pair = keep.astype(jnp.float32) + with_partner(give).astype(jnp.float32)
    tiles = lax.all_to_all(
        pair.astype(jnp.bfloat16), "tp", 0, 0, tiled=True, axis_index_groups=same_core()
    )
    return jnp.sum(tiles.astype(jnp.float32), axis=0)


def norm_rows(core, mine, other, gain, normed):
    half, length, block = mine.shape
    blocks = CORES * half

    def tile(k):
        return (mine if core == k % CORES else other)[k // CORES].astype(jnp.float32)

    squares = jnp.zeros((length, 1), jnp.float32)
    for k in range(blocks):
        v = tile(k)
        squares = squares + jnp.sum(v * v, axis=-1, keepdims=True)
    inverse = lax.rsqrt(squares / (blocks * block) + 1e-06)
    for k in range(blocks):
        here = slice(k * block, (k + 1) * block)
        normed[:, here] = (tile(k) * inverse * gain[:, here]).astype(jnp.bfloat16)


def put(core, k, value, keep, give):
    (keep if core == k % CORES else give)[k // CORES] = value


def on_each_core(core, body):
    for c in range(CORES):

        @pl.when(core == c)
        def _(c=c):
            body(c)


def parts_of_all_groups(mine):
    groups = lax.axis_size("grp")
    up = [(k, (k + 1) % groups) for k in range(groups)]
    down = [(k, (k - 1) % groups) for k in range(groups)]
    behind = [mine]
    ahead = []
    for _ in range(groups // 2):
        behind.append(lax.ppermute(behind[-1], "grp", up))
    for _ in range((groups - 1) // 2):
        ahead.append(lax.ppermute(ahead[-1] if ahead else mine, "grp", down))
    return behind + ahead[::-1]


def gather_early(shard, waiting):
    rows, cols = shard.shape
    groups = lax.axis_size("grp")
    me = lax.axis_index("grp")
    ring = lax.axis_size("fs")
    runs = ring // RUN
    part = lax.dynamic_slice_in_dim(shard, me * (rows // groups), rows // groups, 0)
    strided = [[k + RUN * j for j in range(runs)] for k in range(RUN)]
    neighbour = [(k, k + 1 - 2 * (k % RUN)) for k in range(ring)]
    level = lax.all_gather(part, "fs", axis=0, tiled=True, axis_index_groups=strided)
    wide = cols // PIECES
    own = [level[:, k * wide : (k + 1) * wide] for k in range(PIECES)]
    near = []
    for k in range(PIECES):
        near.append(lax.ppermute(own[k], "fs", neighbour))
    far = [parts_of_all_groups(own[k]) for k in range(PIECES)]
    beyond = []
    for k in range(PIECES):
        if groups == 2 and k == PIECES - 1:
            beyond.append([near[k], lax.ppermute(far[k][1], "fs", neighbour)])
        else:
            beyond.append(parts_of_all_groups(near[k]))
    return [far[k] + beyond[k] for k in range(PIECES)], waiting


def shifted(x, by, fill):
    rows = lax.broadcasted_iota(jnp.int32, x.shape, 0)
    return jnp.where(rows >= by, pltpu.roll(x, by, 0), fill)


def recurrent_body(groups, pieces, runs, me_ref, *refs):
    taken = pieces * RUN * groups
    parts = refs[:taken]
    mine, other, *small = refs[taken : taken + 8]
    keep, give, normed, weights, *held, landed = refs[taken + 8 :]
    copies = [pltpu.make_async_copy(s, h, landed.at[k]) for k, (s, h) in enumerate(zip(small, held))]
    for copy in copies:
        copy.start()
    gain, taps, decay_map, input_map, base, extra = held
    half, length, block = mine.shape
    blocks = CORES * half
    width = taps.shape[1]
    each = parts[0].shape[0] // runs
    wide = parts[0].shape[1]
    for behind in range(groups):
        place = lax.rem(me_ref[0] + groups - behind, groups) * each
        for side in range(RUN):
            near = lax.rem(me_ref[2] + side, RUN) * groups * each
            for far in range(runs):
                to = pl.multiple_of(far * RUN * groups * each + near + place, each)
                for piece in range(pieces):
                    weights[pl.ds(to, each), piece * wide : (piece + 1) * wide] = parts[
                        (piece * RUN + side) * groups + behind
                    ][far * each : (far + 1) * each, :]
    for copy in copies:
        copy.wait()
    on_each_core(me_ref[1], lambda core: norm_rows(core, mine, other, gain, normed))
    recur = jnp.dot(normed[...], weights[:, :width], preferred_element_type=jnp.float32)
    gate_pre = jnp.dot(
        normed[...], weights[:, width : 2 * width], preferred_element_type=jnp.float32
    )
    gate = jax.nn.gelu(gate_pre).astype(jnp.bfloat16).astype(jnp.float32)
    recur = recur.astype(jnp.bfloat16).astype(jnp.float32)
    count = taps.shape[0]
    conv_sum = recur * taps[count - 1 : count, :].astype(jnp.float32)
    for k in range(1, count):
        conv_sum = conv_sum + shifted(recur, k, 0.0) * taps[count - 1 - k : count - k, :].astype(
            jnp.float32
        )
    conv_rows = conv_sum.astype(jnp.bfloat16)
    count = decay_map.shape[0]
    size = width // count
    recur_gate = []
    input_rate = []
    for k in range(count):
        x = conv_rows[:, k * size : (k + 1) * size]
        recur_gate.append(jnp.dot(x, decay_map[k], preferred_element_type=jnp.float32))
        input_rate.append(jnp.dot(x, input_map[k], preferred_element_type=jnp.float32))
    recur_gate = jax.nn.sigmoid(jnp.concatenate(recur_gate, axis=1))
    input_rate = jax.nn.sigmoid(jnp.concatenate(input_rate, axis=1))
    x = -base[...]
    softplus = jnp.maximum(x, 0.0) + jnp.log1p(jnp.exp(-jnp.abs(x)))
    columns = jnp.broadcast_to(extra[...], (128, length)).T
    columns = jnp.concatenate([columns] * (width // 128), axis=1)
    log_decay = -8.0 * softplus * recur_gate + columns
    decay = jnp.exp(log_decay)
    u = -log_decay
    small = 2.0 * u * (1.0 - u * (1.0 - u * (2.0 / 3.0 - u * (1.0 / 3.0 - u * (2.0 / 15.0)))))
    lost = jnp.where(u < 0.015625, small, 1.0 - decay * decay)
    hidden = jnp.sqrt(lost) * input_rate * conv_rows.astype(jnp.float32)
    by = 1
    while by < length:
        hidden = hidden + decay * shifted(hidden, by, 0.0)
        if 2 * by < length:
            decay = decay * shifted(decay, by, 1.0)
        by *= 2
    mixed = (hidden * gate).astype(jnp.bfloat16)

    def finish(core):
        for k in range(blocks):
            product = lax.dot_general(
                mixed,
                weights[k * block : (k + 1) * block, 2 * width : 3 * width],
                (((1,), (1,)), ((), ())),
                preferred_element_type=jnp.float32,
            )
            put(core, k, product.astype(jnp.bfloat16), keep, give)

    on_each_core(me_ref[1], finish)


def recurrent_block(tiles, parts, gain, taps, decay_gate, input_gate, base, extra):
    groups = len(parts[0]) // RUN
    pieces = len(parts)
    runs = lax.axis_size("fs") // RUN
    place = jnp.stack(
        [lax.axis_index("grp"), lax.axis_index("tp") % CORES, lax.axis_index("fs") % RUN]
    ).astype(jnp.int32)
    small = [gain[None, :], taps, decay_gate, input_gate, base[None, :], extra[None, :]]
    flat = [p for piece in parts for p in piece]
    half, length, block = tiles[0].shape
    vmem = pl.BlockSpec(memory_space=pltpu.VMEM)
    features = CORES * half * block
    cols = pieces * parts[0][0].shape[1]
    return pl.pallas_call(
        lambda *refs: recurrent_body(groups, pieces, runs, *refs),
        out_shape=[jax.ShapeDtypeStruct(tiles[0].shape, jnp.bfloat16)] * 2,
        in_specs=[pl.BlockSpec(memory_space=pltpu.SMEM)] + [vmem] * (len(flat) + 2)
        + [pl.BlockSpec(memory_space=pltpu.HBM)] * len(small),
        out_specs=[vmem] * 2,
        scratch_shapes=[
            pltpu.VMEM((length, features), jnp.bfloat16),
            pltpu.VMEM((features, cols), jnp.bfloat16),
            *[pltpu.VMEM(s.shape, s.dtype) for s in small],
            pltpu.SemaphoreType.DMA((len(small),)),
        ],
        cost_estimate=pl.CostEstimate(
            flops=2 * length * features * cols,
            transcendentals=6 * length * taps.shape[1],
            bytes_accessed=2 * (features * cols + 2 * length * features),
        ),
        compiler_params=pltpu.CompilerParams(vmem_limit_bytes=40 << 20),
        name="recurrent",
    )(
        place,
        *flat,
        *tiles,
        *[pltpu.with_memory_space_constraint(s, pltpu.HBM) for s in small],
    )


def feed_forward_body(
    core_ref, mine, other, gain, weights, keep, give, normed, squared, up, down, arrived
):
    half, _, block = mine.shape
    blocks = CORES * half
    hidden = squared.shape[1]
    chunks = hidden // CHUNK
    ups = [
        pltpu.make_async_copy(weights.at[:, k * CHUNK : (k + 1) * CHUNK], up.at[k], arrived.at[k])
        for k in range(chunks)
    ]
    downs = [
        pltpu.make_async_copy(
            weights.at[k * block : (k + 1) * block, hidden:], down.at[k], arrived.at[chunks + k]
        )
        for k in range(blocks)
    ]
    for copy in ups + downs:
        copy.start()
    on_each_core(core_ref[0], lambda core: norm_rows(core, mine, other, gain, normed))
    for k in range(chunks):
        ups[k].wait()
        upward = jnp.dot(normed[...], up[k], preferred_element_type=jnp.float32)
        positive = jnp.maximum(upward, 0.0)
        squared[:, k * CHUNK : (k + 1) * CHUNK] = (positive * positive).astype(jnp.bfloat16)
    for copy in downs:
        copy.wait()

    def finish(core):
        for k in range(blocks):
            product = lax.dot_general(
                squared[...],
                down[k],
                (((1,), (1,)), ((), ())),
                preferred_element_type=jnp.float32,
            )
            put(core, k, product.astype(jnp.bfloat16), keep, give)

    on_each_core(core_ref[0], finish)


def feed_forward(tiles, gain, weights):
    _, length, block = tiles[0].shape
    features, both = weights.shape
    hidden = both // 2
    chunks = hidden // CHUNK
    vmem = pl.BlockSpec(memory_space=pltpu.VMEM)
    core = (lax.axis_index("tp") % CORES).astype(jnp.int32).reshape(1)
    return pl.pallas_call(
        feed_forward_body,
        out_shape=[jax.ShapeDtypeStruct(tiles[0].shape, jnp.bfloat16)] * 2,
        in_specs=[
            pl.BlockSpec(memory_space=pltpu.SMEM),
            vmem,
            vmem,
            vmem,
            pl.BlockSpec(memory_space=pltpu.HBM),
        ],
        out_specs=[vmem] * 2,
        scratch_shapes=[
            pltpu.VMEM((length, features), jnp.bfloat16),
            pltpu.VMEM((length, hidden), jnp.bfloat16),
            pltpu.VMEM((chunks, features, CHUNK), jnp.bfloat16),
            pltpu.VMEM((features // block, block, hidden), jnp.bfloat16),
            pltpu.SemaphoreType.DMA((chunks + features // block,)),
        ],
        cost_estimate=pl.CostEstimate(
            flops=2 * length * features * both,
            transcendentals=length,
            bytes_accessed=2 * (features * both + 2 * length * features),
        ),
        compiler_params=pltpu.CompilerParams(vmem_limit_bytes=40 << 20),
        name="feed_forward",
    )(core, *tiles, gain[None, :], pltpu.with_memory_space_constraint(weights, pltpu.HBM))


def per_device(
    tokens,
    recurrent_norm_gain,
    feedforward_norm_gain,
    gate_projection_weight,
    recurrent_projection_weight,
    convolution_kernel,
    decay_gate_matrix,
    input_gate_matrix,
    base_decay_logit,
    extra_log_decay,
    output_projection_weight,
    up_projection_weight,
    down_projection_weight,
):
    late = jnp.concatenate([up_projection_weight, down_projection_weight.T], axis=1)
    late, tokens = lax.optimization_barrier((late, tokens))
    late_whole = lax.all_gather(late, "fs", axis=0, tiled=True)
    early = jnp.concatenate(
        [recurrent_projection_weight, gate_projection_weight, output_projection_weight.T], axis=1
    )
    parts, held = gather_early(early, tokens)
    token_tiles = from_everyone(held)
    keep, give = recurrent_block(
        token_tiles,
        parts,
        recurrent_norm_gain,
        convolution_kernel,
        decay_gate_matrix,
        input_gate_matrix,
        base_decay_logit,
        extra_log_decay,
    )
    residual = (tokens.astype(jnp.float32) + summed_over_peers(keep, give)).astype(jnp.bfloat16)
    keep, give = feed_forward(from_everyone(residual), feedforward_norm_gain, late_whole)
    return (residual.astype(jnp.float32) + summed_over_peers(keep, give)).astype(jnp.bfloat16)


def solution(mesh):
    placed = (
        P(("grp", "fs"), "tp"),
        P(),
        P(),
        P("fs", "tp"),
        P("fs", "tp"),
        P(None, "tp"),
        P("tp", None, None),
        P("tp", None, None),
        P("tp"),
        P(("grp", "fs")),
        P("tp", "fs"),
        P("fs", "tp"),
        P("tp", "fs"),
    )

    return jax.shard_map(
        per_device, mesh=mesh, in_specs=placed, out_specs=P(("grp", "fs"), "tp"), check_vma=False
    )
```

```python
import jax
import jax.numpy as jnp
from jax import lax
from jax.experimental import pallas as pl
from jax.experimental.pallas import tpu as pltpu
from jax.sharding import PartitionSpec as P


RUN = 2
CORES = 2
CHUNK = 256
PIECES = 2


def same_core():
    members = lax.axis_size("tp")
    return [list(range(c, members, CORES)) for c in range(CORES)]


def with_partner(x):
    members = lax.axis_size("tp")
    return lax.ppermute(x, "tp", [(k, k + 1 - 2 * (k % CORES)) for k in range(members)])


def from_everyone(x):
    groups = same_core()
    copies = jnp.broadcast_to(x, (len(groups[0]), *x.shape))
    mine = lax.all_to_all(copies, "tp", 0, 0, tiled=True, axis_index_groups=groups)
    return mine, with_partner(mine)


def summed_over_peers(keep, give):
    pair = keep.astype(jnp.float32) + with_partner(give).astype(jnp.float32)
    tiles = lax.all_to_all(
        pair.astype(jnp.bfloat16), "tp", 0, 0, tiled=True, axis_index_groups=same_core()
    )
    return jnp.sum(tiles.astype(jnp.float32), axis=0)


def norm_rows(core, mine, other, gain, normed):
    half, length, block = mine.shape
    blocks = CORES * half

    def tile(k):
        return (mine if core == k % CORES else other)[k // CORES].astype(jnp.float32)

    squares = jnp.zeros((length, 1), jnp.float32)
    for k in range(blocks):
        v = tile(k)
        squares = squares + jnp.sum(v * v, axis=-1, keepdims=True)
    inverse = lax.rsqrt(squares / (blocks * block) + 1e-06)
    for k in range(blocks):
        here = slice(k * block, (k + 1) * block)
        normed[:, here] = (tile(k) * inverse * gain[:, here]).astype(jnp.bfloat16)


def put(core, k, value, keep, give):
    (keep if core == k % CORES else give)[k // CORES] = value


def on_each_core(core, body):
    for c in range(CORES):

        @pl.when(core == c)
        def _(c=c):
            body(c)


def parts_of_all_groups(mine):
    groups = lax.axis_size("grp")
    up = [(k, (k + 1) % groups) for k in range(groups)]
    down = [(k, (k - 1) % groups) for k in range(groups)]
    behind = [mine]
    ahead = []
    for _ in range(groups // 2):
        behind.append(lax.ppermute(behind[-1], "grp", up))
    for _ in range((groups - 1) // 2):
        ahead.append(lax.ppermute(ahead[-1] if ahead else mine, "grp", down))
    return behind + ahead[::-1]


def gather_early(shard, waiting):
    rows, cols = shard.shape
    groups = lax.axis_size("grp")
    me = lax.axis_index("grp")
    ring = lax.axis_size("fs")
    runs = ring // RUN
    part = lax.dynamic_slice_in_dim(shard, me * (rows // groups), rows // groups, 0)
    strided = [[k + RUN * j for j in range(runs)] for k in range(RUN)]
    turns = [[(k, (k + way) % ring) for k in range(ring)] for way in (1, -1)]
    level = lax.all_gather(part, "fs", axis=0, tiled=True, axis_index_groups=strided)
    wide = cols // PIECES
    own = [level[:, k * wide : (k + 1) * wide] for k in range(PIECES)]
    near = []
    for k in range(PIECES):
        near.append(lax.ppermute(own[k], "fs", turns[k % 2]))
    far = [parts_of_all_groups(own[k]) for k in range(PIECES)]
    beyond = [parts_of_all_groups(near[k]) for k in range(PIECES)]
    return [far[k] + beyond[k] for k in range(PIECES)], waiting


def shifted(x, by, fill):
    rows = lax.broadcasted_iota(jnp.int32, x.shape, 0)
    return jnp.where(rows >= by, pltpu.roll(x, by, 0), fill)


def recurrent_body(groups, pieces, runs, me_ref, *refs):
    taken = pieces * RUN * groups
    parts = refs[:taken]
    mine, other, *small = refs[taken : taken + 8]
    keep, give, normed, weights, *held, landed = refs[taken + 8 :]
    copies = [pltpu.make_async_copy(s, h, landed.at[k]) for k, (s, h) in enumerate(zip(small, held))]
    for copy in copies:
        copy.start()
    gain, taps, decay_map, input_map, base, extra = held
    half, length, block = mine.shape
    blocks = CORES * half
    width = taps.shape[1]
    each = parts[0].shape[0] // runs
    wide = parts[0].shape[1]
    for behind in range(groups):
        place = lax.rem(me_ref[0] + groups - behind, groups) * each
        for side in range(RUN):
            near = lax.rem(me_ref[2] + side, RUN) * groups * each
            for far in range(runs):
                to = pl.multiple_of(far * RUN * groups * each + near + place, each)
                for piece in range(pieces):
                    weights[pl.ds(to, each), piece * wide : (piece + 1) * wide] = parts[
                        (piece * RUN + side) * groups + behind
                    ][far * each : (far + 1) * each, :]
    for copy in copies:
        copy.wait()
    on_each_core(me_ref[1], lambda core: norm_rows(core, mine, other, gain, normed))
    recur = jnp.dot(normed[...], weights[:, :width], preferred_element_type=jnp.float32)
    gate_pre = jnp.dot(
        normed[...], weights[:, width : 2 * width], preferred_element_type=jnp.float32
    )
    gate = jax.nn.gelu(gate_pre).astype(jnp.bfloat16).astype(jnp.float32)
    recur = recur.astype(jnp.bfloat16).astype(jnp.float32)
    count = taps.shape[0]
    conv_sum = recur * taps[count - 1 : count, :].astype(jnp.float32)
    for k in range(1, count):
        conv_sum = conv_sum + shifted(recur, k, 0.0) * taps[count - 1 - k : count - k, :].astype(
            jnp.float32
        )
    conv_rows = conv_sum.astype(jnp.bfloat16)
    count = decay_map.shape[0]
    size = width // count
    recur_gate = []
    input_rate = []
    for k in range(count):
        x = conv_rows[:, k * size : (k + 1) * size]
        recur_gate.append(jnp.dot(x, decay_map[k], preferred_element_type=jnp.float32))
        input_rate.append(jnp.dot(x, input_map[k], preferred_element_type=jnp.float32))
    recur_gate = jax.nn.sigmoid(jnp.concatenate(recur_gate, axis=1))
    input_rate = jax.nn.sigmoid(jnp.concatenate(input_rate, axis=1))
    x = -base[...]
    softplus = jnp.maximum(x, 0.0) + jnp.log1p(jnp.exp(-jnp.abs(x)))
    columns = jnp.broadcast_to(extra[...], (128, length)).T
    columns = jnp.concatenate([columns] * (width // 128), axis=1)
    log_decay = -8.0 * softplus * recur_gate + columns
    decay = jnp.exp(log_decay)
    u = -log_decay
    small = 2.0 * u * (1.0 - u * (1.0 - u * (2.0 / 3.0 - u * (1.0 / 3.0 - u * (2.0 / 15.0)))))
    lost = jnp.where(u < 0.015625, small, 1.0 - decay * decay)
    hidden = jnp.sqrt(lost) * input_rate * conv_rows.astype(jnp.float32)
    by = 1
    while by < length:
        hidden = hidden + decay * shifted(hidden, by, 0.0)
        if 2 * by < length:
            decay = decay * shifted(decay, by, 1.0)
        by *= 2
    mixed = (hidden * gate).astype(jnp.bfloat16)

    def finish(core):
        for k in range(blocks):
            product = lax.dot_general(
                mixed,
                weights[k * block : (k + 1) * block, 2 * width : 3 * width],
                (((1,), (1,)), ((), ())),
                preferred_element_type=jnp.float32,
            )
            put(core, k, product.astype(jnp.bfloat16), keep, give)

    on_each_core(me_ref[1], finish)


def recurrent_block(tiles, parts, gain, taps, decay_gate, input_gate, base, extra):
    groups = len(parts[0]) // RUN
    pieces = len(parts)
    runs = lax.axis_size("fs") // RUN
    place = jnp.stack(
        [lax.axis_index("grp"), lax.axis_index("tp") % CORES, lax.axis_index("fs") % RUN]
    ).astype(jnp.int32)
    small = [gain[None, :], taps, decay_gate, input_gate, base[None, :], extra[None, :]]
    flat = [p for piece in parts for p in piece]
    half, length, block = tiles[0].shape
    vmem = pl.BlockSpec(memory_space=pltpu.VMEM)
    features = CORES * half * block
    cols = pieces * parts[0][0].shape[1]
    return pl.pallas_call(
        lambda *refs: recurrent_body(groups, pieces, runs, *refs),
        out_shape=[jax.ShapeDtypeStruct(tiles[0].shape, jnp.bfloat16)] * 2,
        in_specs=[pl.BlockSpec(memory_space=pltpu.SMEM)] + [vmem] * (len(flat) + 2)
        + [pl.BlockSpec(memory_space=pltpu.HBM)] * len(small),
        out_specs=[vmem] * 2,
        scratch_shapes=[
            pltpu.VMEM((length, features), jnp.bfloat16),
            pltpu.VMEM((features, cols), jnp.bfloat16),
            *[pltpu.VMEM(s.shape, s.dtype) for s in small],
            pltpu.SemaphoreType.DMA((len(small),)),
        ],
        cost_estimate=pl.CostEstimate(
            flops=2 * length * features * cols,
            transcendentals=6 * length * taps.shape[1],
            bytes_accessed=2 * (features * cols + 2 * length * features),
        ),
        compiler_params=pltpu.CompilerParams(vmem_limit_bytes=40 << 20),
        name="recurrent",
    )(
        place,
        *flat,
        *tiles,
        *[pltpu.with_memory_space_constraint(s, pltpu.HBM) for s in small],
    )


def feed_forward_body(
    core_ref, mine, other, gain, weights, keep, give, normed, squared, up, down, arrived
):
    half, _, block = mine.shape
    blocks = CORES * half
    hidden = squared.shape[1]
    chunks = hidden // CHUNK
    ups = [
        pltpu.make_async_copy(weights.at[:, k * CHUNK : (k + 1) * CHUNK], up.at[k], arrived.at[k])
        for k in range(chunks)
    ]
    downs = [
        pltpu.make_async_copy(
            weights.at[k * block : (k + 1) * block, hidden:], down.at[k], arrived.at[chunks + k]
        )
        for k in range(blocks)
    ]
    for copy in ups + downs:
        copy.start()
    on_each_core(core_ref[0], lambda core: norm_rows(core, mine, other, gain, normed))
    for k in range(chunks):
        ups[k].wait()
        upward = jnp.dot(normed[...], up[k], preferred_element_type=jnp.float32)
        positive = jnp.maximum(upward, 0.0)
        squared[:, k * CHUNK : (k + 1) * CHUNK] = (positive * positive).astype(jnp.bfloat16)
    for copy in downs:
        copy.wait()

    def finish(core):
        for k in range(blocks):
            product = lax.dot_general(
                squared[...],
                down[k],
                (((1,), (1,)), ((), ())),
                preferred_element_type=jnp.float32,
            )
            put(core, k, product.astype(jnp.bfloat16), keep, give)

    on_each_core(core_ref[0], finish)


def feed_forward(tiles, gain, weights):
    _, length, block = tiles[0].shape
    features, both = weights.shape
    hidden = both // 2
    chunks = hidden // CHUNK
    vmem = pl.BlockSpec(memory_space=pltpu.VMEM)
    core = (lax.axis_index("tp") % CORES).astype(jnp.int32).reshape(1)
    return pl.pallas_call(
        feed_forward_body,
        out_shape=[jax.ShapeDtypeStruct(tiles[0].shape, jnp.bfloat16)] * 2,
        in_specs=[
            pl.BlockSpec(memory_space=pltpu.SMEM),
            vmem,
            vmem,
            vmem,
            pl.BlockSpec(memory_space=pltpu.HBM),
        ],
        out_specs=[vmem] * 2,
        scratch_shapes=[
            pltpu.VMEM((length, features), jnp.bfloat16),
            pltpu.VMEM((length, hidden), jnp.bfloat16),
            pltpu.VMEM((chunks, features, CHUNK), jnp.bfloat16),
            pltpu.VMEM((features // block, block, hidden), jnp.bfloat16),
            pltpu.SemaphoreType.DMA((chunks + features // block,)),
        ],
        cost_estimate=pl.CostEstimate(
            flops=2 * length * features * both,
            transcendentals=length,
            bytes_accessed=2 * (features * both + 2 * length * features),
        ),
        compiler_params=pltpu.CompilerParams(vmem_limit_bytes=40 << 20),
        name="feed_forward",
    )(core, *tiles, gain[None, :], pltpu.with_memory_space_constraint(weights, pltpu.HBM))


def per_device(
    tokens,
    recurrent_norm_gain,
    feedforward_norm_gain,
    gate_projection_weight,
    recurrent_projection_weight,
    convolution_kernel,
    decay_gate_matrix,
    input_gate_matrix,
    base_decay_logit,
    extra_log_decay,
    output_projection_weight,
    up_projection_weight,
    down_projection_weight,
):
    late = jnp.concatenate([up_projection_weight, down_projection_weight.T], axis=1)
    late, tokens = lax.optimization_barrier((late, tokens))
    late_whole = lax.all_gather(late, "fs", axis=0, tiled=True)
    early = jnp.concatenate(
        [recurrent_projection_weight, gate_projection_weight, output_projection_weight.T], axis=1
    )
    parts, held = gather_early(early, tokens)
    token_tiles = from_everyone(held)
    keep, give = recurrent_block(
        token_tiles,
        parts,
        recurrent_norm_gain,
        convolution_kernel,
        decay_gate_matrix,
        input_gate_matrix,
        base_decay_logit,
        extra_log_decay,
    )
    residual = (tokens.astype(jnp.float32) + summed_over_peers(keep, give)).astype(jnp.bfloat16)
    keep, give = feed_forward(from_everyone(residual), feedforward_norm_gain, late_whole)
    return (residual.astype(jnp.float32) + summed_over_peers(keep, give)).astype(jnp.bfloat16)


def solution(mesh):
    placed = (
        P(("grp", "fs"), "tp"),
        P(),
        P(),
        P("fs", "tp"),
        P("fs", "tp"),
        P(None, "tp"),
        P("tp", None, None),
        P("tp", None, None),
        P("tp"),
        P(("grp", "fs")),
        P("tp", "fs"),
        P("fs", "tp"),
        P("tp", "fs"),
    )

    return jax.shard_map(
        per_device, mesh=mesh, in_specs=placed, out_specs=P(("grp", "fs"), "tp"), check_vma=False
    )
```

```python
import jax
import jax.numpy as jnp
from jax import lax
from jax.experimental import pallas as pl
from jax.experimental.pallas import tpu as pltpu
from jax.sharding import PartitionSpec as P


RUN = 2
CORES = 2
CHUNK = 256
PIECES = 2


def same_core():
    members = lax.axis_size("tp")
    return [list(range(c, members, CORES)) for c in range(CORES)]


def with_partner(x):
    members = lax.axis_size("tp")
    return lax.ppermute(x, "tp", [(k, k + 1 - 2 * (k % CORES)) for k in range(members)])


def from_everyone(x):
    groups = same_core()
    copies = jnp.broadcast_to(x, (len(groups[0]), *x.shape))
    mine = lax.all_to_all(copies, "tp", 0, 0, tiled=True, axis_index_groups=groups)
    return mine, with_partner(mine)


def summed_over_peers(keep, give):
    pair = keep.astype(jnp.float32) + with_partner(give).astype(jnp.float32)
    tiles = lax.all_to_all(
        pair.astype(jnp.bfloat16), "tp", 0, 0, tiled=True, axis_index_groups=same_core()
    )
    return jnp.sum(tiles.astype(jnp.float32), axis=0)


def norm_rows(core, mine, other, gain, normed):
    half, length, block = mine.shape
    blocks = CORES * half

    def tile(k):
        return (mine if core == k % CORES else other)[k // CORES].astype(jnp.float32)

    squares = jnp.zeros((length, 1), jnp.float32)
    for k in range(blocks):
        v = tile(k)
        squares = squares + jnp.sum(v * v, axis=-1, keepdims=True)
    inverse = lax.rsqrt(squares / (blocks * block) + 1e-06)
    for k in range(blocks):
        here = slice(k * block, (k + 1) * block)
        normed[:, here] = (tile(k) * inverse * gain[:, here]).astype(jnp.bfloat16)


def put(core, k, value, keep, give):
    (keep if core == k % CORES else give)[k // CORES] = value


def on_each_core(core, body):
    for c in range(CORES):

        @pl.when(core == c)
        def _(c=c):
            body(c)


def parts_of_all_groups(mine):
    groups = lax.axis_size("grp")
    up = [(k, (k + 1) % groups) for k in range(groups)]
    down = [(k, (k - 1) % groups) for k in range(groups)]
    behind = [mine]
    ahead = []
    for _ in range(groups // 2):
        behind.append(lax.ppermute(behind[-1], "grp", up))
    for _ in range((groups - 1) // 2):
        ahead.append(lax.ppermute(ahead[-1] if ahead else mine, "grp", down))
    return behind + ahead[::-1]


def gather_early(shard, waiting):
    rows, cols = shard.shape
    groups = lax.axis_size("grp")
    me = lax.axis_index("grp")
    ring = lax.axis_size("fs")
    runs = ring // RUN
    part = lax.dynamic_slice_in_dim(shard, me * (rows // groups), rows // groups, 0)
    strided = [[k + RUN * j for j in range(runs)][:: 1 - 2 * k] for k in range(RUN)]
    turns = [[(k, (k + way) % ring) for k in range(ring)] for way in (1, -1)]
    level = lax.all_gather(part, "fs", axis=0, tiled=True, axis_index_groups=strided)
    wide = cols // PIECES
    own = [level[:, k * wide : (k + 1) * wide] for k in range(PIECES)]
    near = []
    for k in range(PIECES):
        near.append(lax.ppermute(own[k], "fs", turns[k % 2]))
    far = [parts_of_all_groups(own[k]) for k in range(PIECES)]
    beyond = [parts_of_all_groups(near[k]) for k in range(PIECES)]
    return [far[k] + beyond[k] for k in range(PIECES)], waiting


def shifted(x, by, fill):
    rows = lax.broadcasted_iota(jnp.int32, x.shape, 0)
    return jnp.where(rows >= by, pltpu.roll(x, by, 0), fill)


def recurrent_body(groups, pieces, runs, me_ref, *refs):
    taken = pieces * RUN * groups
    parts = refs[:taken]
    mine, other, *small = refs[taken : taken + 8]
    keep, give, normed, weights, *held, landed = refs[taken + 8 :]
    copies = [pltpu.make_async_copy(s, h, landed.at[k]) for k, (s, h) in enumerate(zip(small, held))]
    for copy in copies:
        copy.start()
    gain, taps, decay_map, input_map, base, extra = held
    half, length, block = mine.shape
    blocks = CORES * half
    width = taps.shape[1]
    each = parts[0].shape[0] // runs
    wide = parts[0].shape[1]
    for behind in range(groups):
        place = lax.rem(me_ref[0] + groups - behind, groups) * each
        for side in range(RUN):
            odd = lax.rem(me_ref[2] + side, RUN)
            for far in range(runs):
                at = (far + odd * (runs - 1 - 2 * far)) * RUN + odd
                to = pl.multiple_of(at * groups * each + place, each)
                for piece in range(pieces):
                    weights[pl.ds(to, each), piece * wide : (piece + 1) * wide] = parts[
                        (piece * RUN + side) * groups + behind
                    ][far * each : (far + 1) * each, :]
    for copy in copies:
        copy.wait()
    on_each_core(me_ref[1], lambda core: norm_rows(core, mine, other, gain, normed))
    recur = jnp.dot(normed[...], weights[:, :width], preferred_element_type=jnp.float32)
    gate_pre = jnp.dot(
        normed[...], weights[:, width : 2 * width], preferred_element_type=jnp.float32
    )
    gate = jax.nn.gelu(gate_pre).astype(jnp.bfloat16).astype(jnp.float32)
    recur = recur.astype(jnp.bfloat16).astype(jnp.float32)
    count = taps.shape[0]
    conv_sum = recur * taps[count - 1 : count, :].astype(jnp.float32)
    for k in range(1, count):
        conv_sum = conv_sum + shifted(recur, k, 0.0) * taps[count - 1 - k : count - k, :].astype(
            jnp.float32
        )
    conv_rows = conv_sum.astype(jnp.bfloat16)
    count = decay_map.shape[0]
    size = width // count
    recur_gate = []
    input_rate = []
    for k in range(count):
        x = conv_rows[:, k * size : (k + 1) * size]
        recur_gate.append(jnp.dot(x, decay_map[k], preferred_element_type=jnp.float32))
        input_rate.append(jnp.dot(x, input_map[k], preferred_element_type=jnp.float32))
    recur_gate = jax.nn.sigmoid(jnp.concatenate(recur_gate, axis=1))
    input_rate = jax.nn.sigmoid(jnp.concatenate(input_rate, axis=1))
    x = -base[...]
    softplus = jnp.maximum(x, 0.0) + jnp.log1p(jnp.exp(-jnp.abs(x)))
    columns = jnp.broadcast_to(extra[...], (128, length)).T
    columns = jnp.concatenate([columns] * (width // 128), axis=1)
    log_decay = -8.0 * softplus * recur_gate + columns
    decay = jnp.exp(log_decay)
    u = -log_decay
    small = 2.0 * u * (1.0 - u * (1.0 - u * (2.0 / 3.0 - u * (1.0 / 3.0 - u * (2.0 / 15.0)))))
    lost = jnp.where(u < 0.015625, small, 1.0 - decay * decay)
    hidden = jnp.sqrt(lost) * input_rate * conv_rows.astype(jnp.float32)
    by = 1
    while by < length:
        hidden = hidden + decay * shifted(hidden, by, 0.0)
        if 2 * by < length:
            decay = decay * shifted(decay, by, 1.0)
        by *= 2
    mixed = (hidden * gate).astype(jnp.bfloat16)

    def finish(core):
        for k in range(blocks):
            product = lax.dot_general(
                mixed,
                weights[k * block : (k + 1) * block, 2 * width : 3 * width],
                (((1,), (1,)), ((), ())),
                preferred_element_type=jnp.float32,
            )
            put(core, k, product.astype(jnp.bfloat16), keep, give)

    on_each_core(me_ref[1], finish)


def recurrent_block(tiles, parts, gain, taps, decay_gate, input_gate, base, extra):
    groups = len(parts[0]) // RUN
    pieces = len(parts)
    runs = lax.axis_size("fs") // RUN
    place = jnp.stack(
        [lax.axis_index("grp"), lax.axis_index("tp") % CORES, lax.axis_index("fs") % RUN]
    ).astype(jnp.int32)
    small = [gain[None, :], taps, decay_gate, input_gate, base[None, :], extra[None, :]]
    flat = [p for piece in parts for p in piece]
    half, length, block = tiles[0].shape
    vmem = pl.BlockSpec(memory_space=pltpu.VMEM)
    features = CORES * half * block
    cols = pieces * parts[0][0].shape[1]
    return pl.pallas_call(
        lambda *refs: recurrent_body(groups, pieces, runs, *refs),
        out_shape=[jax.ShapeDtypeStruct(tiles[0].shape, jnp.bfloat16)] * 2,
        in_specs=[pl.BlockSpec(memory_space=pltpu.SMEM)] + [vmem] * (len(flat) + 2)
        + [pl.BlockSpec(memory_space=pltpu.HBM)] * len(small),
        out_specs=[vmem] * 2,
        scratch_shapes=[
            pltpu.VMEM((length, features), jnp.bfloat16),
            pltpu.VMEM((features, cols), jnp.bfloat16),
            *[pltpu.VMEM(s.shape, s.dtype) for s in small],
            pltpu.SemaphoreType.DMA((len(small),)),
        ],
        cost_estimate=pl.CostEstimate(
            flops=2 * length * features * cols,
            transcendentals=6 * length * taps.shape[1],
            bytes_accessed=2 * (features * cols + 2 * length * features),
        ),
        compiler_params=pltpu.CompilerParams(vmem_limit_bytes=40 << 20),
        name="recurrent",
    )(
        place,
        *flat,
        *tiles,
        *[pltpu.with_memory_space_constraint(s, pltpu.HBM) for s in small],
    )


def feed_forward_body(
    core_ref, mine, other, gain, weights, keep, give, normed, squared, up, down, arrived
):
    half, _, block = mine.shape
    blocks = CORES * half
    hidden = squared.shape[1]
    chunks = hidden // CHUNK
    ups = [
        pltpu.make_async_copy(weights.at[:, k * CHUNK : (k + 1) * CHUNK], up.at[k], arrived.at[k])
        for k in range(chunks)
    ]
    downs = [
        pltpu.make_async_copy(
            weights.at[k * block : (k + 1) * block, hidden:], down.at[k], arrived.at[chunks + k]
        )
        for k in range(blocks)
    ]
    for copy in ups + downs:
        copy.start()
    on_each_core(core_ref[0], lambda core: norm_rows(core, mine, other, gain, normed))
    for k in range(chunks):
        ups[k].wait()
        upward = jnp.dot(normed[...], up[k], preferred_element_type=jnp.float32)
        positive = jnp.maximum(upward, 0.0)
        squared[:, k * CHUNK : (k + 1) * CHUNK] = (positive * positive).astype(jnp.bfloat16)
    for copy in downs:
        copy.wait()

    def finish(core):
        for k in range(blocks):
            product = lax.dot_general(
                squared[...],
                down[k],
                (((1,), (1,)), ((), ())),
                preferred_element_type=jnp.float32,
            )
            put(core, k, product.astype(jnp.bfloat16), keep, give)

    on_each_core(core_ref[0], finish)


def feed_forward(tiles, gain, weights):
    _, length, block = tiles[0].shape
    features, both = weights.shape
    hidden = both // 2
    chunks = hidden // CHUNK
    vmem = pl.BlockSpec(memory_space=pltpu.VMEM)
    core = (lax.axis_index("tp") % CORES).astype(jnp.int32).reshape(1)
    return pl.pallas_call(
        feed_forward_body,
        out_shape=[jax.ShapeDtypeStruct(tiles[0].shape, jnp.bfloat16)] * 2,
        in_specs=[
            pl.BlockSpec(memory_space=pltpu.SMEM),
            vmem,
            vmem,
            vmem,
            pl.BlockSpec(memory_space=pltpu.HBM),
        ],
        out_specs=[vmem] * 2,
        scratch_shapes=[
            pltpu.VMEM((length, features), jnp.bfloat16),
            pltpu.VMEM((length, hidden), jnp.bfloat16),
            pltpu.VMEM((chunks, features, CHUNK), jnp.bfloat16),
            pltpu.VMEM((features // block, block, hidden), jnp.bfloat16),
            pltpu.SemaphoreType.DMA((chunks + features // block,)),
        ],
        cost_estimate=pl.CostEstimate(
            flops=2 * length * features * both,
            transcendentals=length,
            bytes_accessed=2 * (features * both + 2 * length * features),
        ),
        compiler_params=pltpu.CompilerParams(vmem_limit_bytes=40 << 20),
        name="feed_forward",
    )(core, *tiles, gain[None, :], pltpu.with_memory_space_constraint(weights, pltpu.HBM))


def per_device(
    tokens,
    recurrent_norm_gain,
    feedforward_norm_gain,
    gate_projection_weight,
    recurrent_projection_weight,
    convolution_kernel,
    decay_gate_matrix,
    input_gate_matrix,
    base_decay_logit,
    extra_log_decay,
    output_projection_weight,
    up_projection_weight,
    down_projection_weight,
):
    late = jnp.concatenate([up_projection_weight, down_projection_weight.T], axis=1)
    late, tokens = lax.optimization_barrier((late, tokens))
    late_whole = lax.all_gather(late, "fs", axis=0, tiled=True)
    early = jnp.concatenate(
        [recurrent_projection_weight, gate_projection_weight, output_projection_weight.T], axis=1
    )
    parts, held = gather_early(early, tokens)
    token_tiles = from_everyone(held)
    keep, give = recurrent_block(
        token_tiles,
        parts,
        recurrent_norm_gain,
        convolution_kernel,
        decay_gate_matrix,
        input_gate_matrix,
        base_decay_logit,
        extra_log_decay,
    )
    residual = (tokens.astype(jnp.float32) + summed_over_peers(keep, give)).astype(jnp.bfloat16)
    keep, give = feed_forward(from_everyone(residual), feedforward_norm_gain, late_whole)
    return (residual.astype(jnp.float32) + summed_over_peers(keep, give)).astype(jnp.bfloat16)


def solution(mesh):
    placed = (
        P(("grp", "fs"), "tp"),
        P(),
        P(),
        P("fs", "tp"),
        P("fs", "tp"),
        P(None, "tp"),
        P("tp", None, None),
        P("tp", None, None),
        P("tp"),
        P(("grp", "fs")),
        P("tp", "fs"),
        P("fs", "tp"),
        P("tp", "fs"),
    )

    return jax.shard_map(
        per_device, mesh=mesh, in_specs=placed, out_specs=P(("grp", "fs"), "tp"), check_vma=False
    )
```
